256 devices in a mesh: sp: 64 (over z, y, core), tp: 4 (over x).
Axes of the slice: x: 4, y: 4, z: 8, core: 2. Of those that a mesh axis runs over, the one named last changes fastest.
Arguments:
- out_grad: bfloat16 [8192, 2048], P('sp'), may hold values from -16 to 16
- residual: bfloat16 [8192, 2048], P('sp'), may hold values from -6 to 6
- routes: int32 [8192, 2], P('sp'), may hold values from 0 to 31, all different within a row; in each aligned block of 128 rows (0 to 127, 128 to 255, ...) at most 10 rows name the same one
- route_weights: float32 [8192, 2], P('sp'), may hold values from 0.15 to 0.85, as said below
- w_gate: bfloat16 [64, 2048, 2048], P('sp', None, 'tp'), may hold values from -0.125 to 0.125
- w_up: bfloat16 [64, 2048, 2048], P('sp', None, 'tp'), may hold values from -0.125 to 0.125
- w_down: bfloat16 [64, 2048, 2048], P('sp', 'tp'), may hold values from -0.09375 to 0.09375
- out_gate: bfloat16 [8192, 1024], P('sp', 'tp'), may hold values from -6 to 6
- in_gate: bfloat16 [8192, 1024], P('sp', 'tp'), may hold values from -6 to 6
- conv_input: bfloat16 [8192, 1024], P('sp', 'tp'), may hold values from -6 to 6
- conv_out: bfloat16 [8192, 1024], P('sp', 'tp'), may hold values from -6 to 6
- conv_taps: float32 [3, 1024], P(None, 'tp'), may hold values from -3.5 to 3.5
- w_out: bfloat16 [1024, 2048], P('tp'), may hold values from -0.1875 to 0.1875
Outputs:
- grad_resid: bfloat16 [8192, 2048], P('sp')
- grad_up: bfloat16 [64, 2048, 2048], P('sp', None, 'tp')
- grad_down: bfloat16 [64, 2048, 2048], P('sp', 'tp')
- grad_out_gate: bfloat16 [8192, 1024], P('sp', 'tp')
- grad_in_gate: bfloat16 [8192, 1024], P('sp', 'tp')
- grad_conv_input: bfloat16 [8192, 1024], P('sp', 'tp')
- grad_w_out: float32 [2048, 1024], P('sp', 'tp')
The draws below stay inside these ranges and needn't reach their ends.
Inputs may be any that keep to these rules, and one draw needn't show every extreme that they name: `routes`: each row names 2 different experts. In the rows of one index of sp no expert is named more than 10 times, a bound that some block reaches. `route_weights`: the two weights of a row sum to one.
All inputs are finite; a program needn't handle non-finite values.
Results may differ from the reference program's by a relative error of at most 0.013.
Values may be sent and summed in bfloat16 or wider, within the bound.
A program may use at most 128 MiB of HBM per device.

```python
import math
import jax
import jax.numpy as jnp
import numpy as np
from jax import lax

D = 2048
FF_HALF = 2048
SC = 1024
TOP_K = 2
TOK_DEV = 128
TOKENS = 8192
EXPERTS = 32
SLICES = 64
CAP = 10
N_SP = 64
N_TP = 4


def draw_route_weights(key, part):
    leading = jax.random.uniform(key, (TOKENS, 1), jnp.float32, 0.15, 0.85)
    return jnp.concatenate([leading, 1.0 - leading], axis=1)


def with_spikes(array, key, source, target, shards_of, factor):
    owner, partner = [(jnp.arange(array.shape[dim]) // (array.shape[dim] // shards_of)).reshape([-1 if axis == dim else 1 for axis in range(array.ndim)]) for dim in (source, target)]
    chosen = jax.random.permutation(key, shards_of)[partner]
    strong = (owner == chosen) | (owner == (partner + shards_of // 2) % shards_of)
    return jnp.where(strong, factor * array, array)


def steps_of(rng, dims, pieces, least, largest):
    factor_of, own = 1.0, jax.random.fold_in(rng, 6)
    for position, parts in pieces:
        draws = jnp.exp(jax.random.uniform(jax.random.fold_in(own, position), (parts,), jnp.float32, least / len(pieces), largest / len(pieces)))
        factor_of = factor_of * jnp.repeat(draws, dims[position] // parts).reshape([-1 if axis == position else 1 for axis in range(len(dims))])
    return factor_of


def shared_out(own_key, own, number, rows, count, top, reach, lean):
    order = jax.random.permutation(own_key, count)
    heavy_load, usual = load_shares(count, rows * top, reach, lean, True), load_shares(count, rows * top, reach, lean, False)
    places = jnp.arange(count)

    def named(tallies, rotation):
        used = int((tallies > 0).sum())
        fixed = max(1, used // 4)
        passed = fixed + (places - fixed + rotation * (used - fixed)) % max(1, count - fixed)
        return jnp.zeros((count,), jnp.int32).at[order[jnp.where(places < fixed, places, passed)]].set(jnp.asarray(tallies, jnp.int32))

    tallies = jnp.where(number % 4 == 0, named(heavy_load, number // 4), named(usual, number - number // 4 - 1))
    mixed = jax.random.permutation(jax.random.fold_in(own, 3), count)
    source_of, receiver = mixed[0:count // 2 * 2:2], mixed[1:count // 2 * 2:2]
    slack = jnp.minimum(tallies[source_of] - 1, reach - tallies[receiver]) // 2
    slack = jnp.where((source_of == order[0]) | (receiver == order[0]) | (tallies[receiver] == 0), 0, jnp.maximum(slack, 0))
    passed = jax.random.randint(jax.random.fold_in(own, 4), (count // 2,), 0, 1 << 20) % (slack + 1)
    tallies = tallies.at[source_of].add(-passed).at[receiver].add(passed)
    members = jnp.searchsorted(jnp.cumsum(tallies), jnp.arange(rows * top), side="right").astype(jnp.int32)
    grid = members.reshape(top, rows).T
    grid = grid[jax.random.permutation(jax.random.fold_in(own, 1), rows)]
    rotation = jax.random.randint(jax.random.fold_in(own, 2), (rows, 1), 0, top)
    return jnp.take_along_axis(grid, (jnp.arange(top)[None, :] + rotation) % top, axis=1)


def load_shares(amount, total, reach, slope, full):
    portions = [(1 << 20) // math.isqrt(grade ** slope) + 1 for grade in range(1, amount + 1)]
    largest = reach if full else min(reach, max(-(-total // amount), total * portions[0] // sum(portions)))
    least = 1 if total - largest >= amount - 1 else 0
    counts, surplus = [largest] + [least] * (amount - 1), total - largest - least * (amount - 1)
    while surplus > 0:
        candidates = [i for i in range(1, amount) if counts[i] < largest] or [i for i in range(1, amount) if counts[i] < reach]
        whole, remaining = sum([portions[i] for i in candidates]), surplus
        for i in candidates:
            addition = min(reach - counts[i], max(1, remaining * portions[i] // whole), surplus)
            counts[i] = counts[i] + addition
            surplus = surplus - addition
    return np.array(counts)


def scatter_about(key, shape, scale, limit, pieces=(), held_as=jnp.bfloat16):
    entries = scale * jax.random.normal(key, shape, jnp.float32)
    if pieces:
        entries = entries * steps_of(key, shape, pieces, -0.22, 0.18)
    return jnp.clip(entries, -limit, limit).astype(held_as)


def noise_with(stream_key, dims, spread, reach, shards, heavy, kind=jnp.bfloat16):
    entries = spread * jax.random.normal(stream_key, dims, jnp.float32)
    if shards:
        entries = entries * steps_of(stream_key, dims, shards, -0.22, 0.18)
    return jnp.clip(with_spikes(entries, jax.random.fold_in(stream_key, 3), *heavy), -reach, reach).astype(kind)


def setup_inputs(seed: int = 0) -> dict:
    keys = jax.random.split(jax.random.key(seed), 14)
    out_grad = noise_with(keys[0], (TOKENS, D), 1.0, 16.0, ((0, 64),), (0, 1, 64, 4.0))
    residual = scatter_about(keys[1], (TOKENS, D), 1.0, 6.0, ((0, 64),))
    routes_keys = jax.random.split(jax.random.fold_in(keys[2], 1), TOKENS // TOK_DEV)
    routes_turns = jax.random.permutation(jax.random.fold_in(keys[2], 3), TOKENS // TOK_DEV)
    routes = jax.vmap(lambda own, number: shared_out(jax.random.fold_in(keys[2], 2), own, number, TOK_DEV, EXPERTS, TOP_K, CAP, 1))(routes_keys, routes_turns).reshape((TOKENS, TOP_K))
    route_weights = draw_route_weights(jax.random.fold_in(keys[13], 71), 0)
    w_gate = scatter_about(keys[4], (SLICES, D, FF_HALF), D ** -0.5, 0.125, ((0, 64), (2, 4)))
    w_up = scatter_about(keys[5], (SLICES, D, FF_HALF), D ** -0.5, 0.125, ((0, 64), (2, 4)))
    w_down = scatter_about(keys[6], (SLICES, FF_HALF, D), (2 * FF_HALF) ** -0.5, 0.09375, ((0, 64), (1, 4)))
    out_gate = scatter_about(keys[7], (TOKENS, SC), 1.0, 6.0, ((0, 64), (1, 4)))
    in_gate = scatter_about(keys[8], (TOKENS, SC), 1.0, 6.0, ((0, 64), (1, 4)))
    conv_input = scatter_about(keys[9], (TOKENS, SC), 1.0, 6.0, ((0, 64), (1, 4)))
    conv_out = scatter_about(keys[10], (TOKENS, SC), 1.0, 6.0, ((0, 64), (1, 4)))
    conv_taps = scatter_about(keys[11], (3, SC), 3 ** -0.5, 3.5, ((1, 4),), jnp.float32)
    w_out = scatter_about(keys[12], (SC, D), SC ** -0.5, 0.1875, ((0, 4),))
    return dict(out_grad=out_grad, residual=residual, routes=routes, route_weights=route_weights, w_gate=w_gate, w_up=w_up, w_down=w_down, out_gate=out_gate, in_gate=in_gate, conv_input=conv_input, conv_out=conv_out, conv_taps=conv_taps, w_out=w_out)


epsilon = 1e-06

def reference(out_grad, residual, routes, route_weights, w_gate, w_up, w_down, out_gate, in_gate, conv_input, conv_out, conv_taps, w_out):
    resid_f32 = residual.astype(jnp.float32)
    inv_rms = lax.rsqrt(lax.optimization_barrier(jnp.mean(resid_f32 * resid_f32, axis=-1, keepdims=True)) + epsilon)
    unit_rows = resid_f32 * inv_rms
    normed = unit_rows.astype(jnp.bfloat16)
    n_assign = TOKENS * TOP_K
    weighted = (route_weights[:, :, None] * out_grad.astype(jnp.float32)[:, None, :]).astype(jnp.bfloat16).reshape(n_assign, D)
    flat_routes = routes.reshape(-1).astype(jnp.int32)
    onehot = (flat_routes[:, None] == jnp.arange(EXPERTS, dtype=jnp.int32)[None, :]).astype(jnp.int32)
    blocks = onehot.reshape(N_SP, TOP_K * TOK_DEV, EXPERTS)
    before = (jnp.cumsum(blocks, axis=1) - blocks).reshape(n_assign, EXPERTS)
    slot_rank = lax.optimization_barrier(jnp.sum(before * onehot, axis=1)).astype(jnp.int32)
    source = (jnp.arange(n_assign, dtype=jnp.int32) // (TOP_K * TOK_DEV)).astype(jnp.int32)
    slot_table = jnp.full((EXPERTS, N_SP * CAP), n_assign, jnp.int32)
    slot_table = slot_table.at[flat_routes, source * CAP + slot_rank].set(jnp.arange(n_assign, dtype=jnp.int32))
    quarter = FF_HALF // N_TP
    n_blocks = 2 * N_TP

    def one_expert(expert):
        slot_ids = slot_table[expert]
        filled = slot_ids < n_assign
        safe_ids = jnp.where(filled, slot_ids, 0)
        expert_rows = jnp.where(filled[:, None], normed[safe_ids // TOP_K], jnp.zeros((), jnp.bfloat16))
        expert_grads = jnp.where(filled[:, None], weighted[safe_ids], jnp.zeros((), jnp.bfloat16))
        gate_full = jnp.concatenate([w_gate[2 * expert], w_gate[2 * expert + 1]], axis=1)
        up_full = jnp.concatenate([w_up[2 * expert], w_up[2 * expert + 1]], axis=1)
        down_full = jnp.concatenate([w_down[2 * expert], w_down[2 * expert + 1]], axis=0)
        pre_gate = jnp.dot(expert_rows, gate_full, preferred_element_type=jnp.float32)
        pre_up = jnp.dot(expert_rows, up_full, preferred_element_type=jnp.float32)
        sigmoid_gate = jax.nn.sigmoid(pre_gate)
        activated = pre_gate * sigmoid_gate
        hidden = (activated * pre_up).astype(jnp.bfloat16)
        d_hidden = jnp.dot(expert_grads, down_full.T, preferred_element_type=jnp.float32)
        grad_down = jnp.dot(hidden.T, expert_grads, preferred_element_type=jnp.float32).astype(jnp.bfloat16)
        d_gate = (d_hidden * pre_up * sigmoid_gate * (1.0 + pre_gate * (1.0 - sigmoid_gate))).astype(jnp.bfloat16)
        d_up = (d_hidden * activated).astype(jnp.bfloat16)
        grad_up = jnp.dot(expert_rows.T, d_up, preferred_element_type=jnp.float32).astype(jnp.bfloat16)
        partial_value = jnp.einsum('rjf,djf->jrd', d_gate.astype(jnp.float32).reshape(-1, n_blocks, quarter), gate_full.astype(jnp.float32).reshape(D, n_blocks, quarter))
        partial_value = partial_value + jnp.einsum('rjf,djf->jrd', d_up.astype(jnp.float32).reshape(-1, n_blocks, quarter), up_full.astype(jnp.float32).reshape(D, n_blocks, quarter))
        partial_value = lax.optimization_barrier(partial_value.astype(jnp.bfloat16)).astype(jnp.float32)
        slice_sum = lax.optimization_barrier(jnp.sum(partial_value.reshape(2, N_TP, -1, D), axis=1)).astype(jnp.bfloat16)
        down_pair = grad_down.reshape(2, FF_HALF, D)
        up_pair = jnp.transpose(grad_up.reshape(D, 2, FF_HALF), (1, 0, 2))
        return (down_pair, up_pair, slice_sum, slot_ids)
    down_all, up_all, sums_all, ids_all = lax.map(one_expert, jnp.arange(EXPERTS, dtype=jnp.int32))
    grad_down = down_all.reshape(SLICES, FF_HALF, D)
    grad_up = up_all.reshape(SLICES, D, FF_HALF)
    contrib = lax.optimization_barrier(jnp.sum(sums_all.astype(jnp.float32), axis=1)).reshape(-1, D)
    collected = jnp.zeros((n_assign + 1, D), jnp.float32).at[ids_all.reshape(-1)].add(contrib)
    d_normed = lax.optimization_barrier(jnp.sum(collected[:n_assign].reshape(TOKENS, TOP_K, D), axis=1))
    row_mean = lax.optimization_barrier(jnp.mean(unit_rows * d_normed, axis=-1, keepdims=True))
    grad_resid = (out_grad.astype(jnp.float32) + inv_rms * (d_normed - unit_rows * row_mean)).astype(jnp.bfloat16)
    d_mix = jnp.dot(grad_resid, w_out.T, preferred_element_type=jnp.float32)
    conv_f32 = conv_out.astype(jnp.float32)
    gate_f32 = out_gate.astype(jnp.float32)
    grad_out_gate = (d_mix * conv_f32).astype(jnp.bfloat16)
    d_conv = d_mix * gate_f32
    padded = jnp.pad(d_conv, ((1, 1), (0, 0)))
    taps_f32 = conv_taps.astype(jnp.float32)
    d_inner = taps_f32[0] * padded[2:] + taps_f32[1] * padded[1:-1] + taps_f32[2] * padded[:-2]
    grad_in_gate = (d_inner * conv_input.astype(jnp.float32)).astype(jnp.bfloat16)
    grad_conv_input = (d_inner * in_gate.astype(jnp.float32)).astype(jnp.bfloat16)
    mixed = (gate_f32 * conv_f32).astype(jnp.bfloat16)
    grad_w_out = jnp.dot(grad_resid.T, mixed, preferred_element_type=jnp.float32)
    return (grad_resid, grad_up, grad_down, grad_out_gate, grad_in_gate, grad_conv_input, grad_w_out)
```

```python
import jax
import jax.numpy as jnp
import numpy as np
from jax import lax
from jax.experimental import pallas as pl
from jax.experimental.pallas import tpu as pltpu
from jax.sharding import PartitionSpec as P

MESH = pl.DeviceIdType.MESH
EPS = 1e-06
F32 = jnp.float32
BF16 = jnp.bfloat16

D = 2048
H = 512
Q = 512
TOK = 128
CAP = 10
NZ, NY, NX = 8, 4, 4
CHIPS = NZ * NY
MSG = 4 * CAP
GROUPS = 4
GROW = 8 * CAP
HALF = GROUPS * GROW
C = 256
Z_ORDER = (0, 1, 7, 2, 6, 3, 5, 4)
O_OFF = (2, 1, 3, 0)


def permutation():
    place = np.zeros((8 * MSG, 8 * MSG), np.float32)
    for part in range(4):
        for source in range(8):
            for slot in range(CAP):
                place[part * GROW + source * CAP + slot, source * MSG + part * CAP + slot] = 1
    return place


def nt(a, b):
    return lax.dot_general(a, b, (((1,), (1,)), ((), ())), preferred_element_type=F32)


def tn(a, b):
    return lax.dot_general(a, b, (((0,), (0,)), ((), ())), preferred_element_type=F32)


def nn(a, b):
    return jnp.dot(a, b, preferred_element_type=F32)


def m8(value, by=8):
    return pl.multiple_of(value, by)


def kernel(
    og, resid, routes, rw, wg_h, wu_h, wd_h, ogate, igate, cin, cout, taps, wout, perm, perm_t,
    gr_o, gup_o, gdn_o, gog_o, gig_o, gci_o, gwo_o,
    wg, wu, wd, s_buf, r_buf, xa, hid, dga, dup, ps, pr, po, ra, rb, rc, rd, cs, rt, bk, dn,
    gacc, gb, gp, gs, g_in, dcv, hp, hn, gup, gdn,
    w_sem, loc_sem, pl_s, pl_r, rt_s, rt_r, g_s, g_r, xs, xr, q_s, q_r, e_s, e_r, dn_s, dn_r, t_s, t_r, out_sem,
):
    s = lax.axis_index("sp")
    x = lax.axis_index("tp")
    c = s // 2
    k = s % 2
    z = c // NY
    y = c % NY
    right = (s, (x + 1) % NX)
    left = (s, (x + 3) % NX)
    mate = (2 * c + 1 - k, x)
    before = ((s + 63) % 64, x)
    after = ((s + 1) % 64, x)
    across = ((s + 63 + 2 * k) % 64, x)

    def expert_of(i, dy):
        return ((z + NZ - Z_ORDER[i]) % NZ) * NY + (y + dy) % NY

    def source_of(p):
        return ((z + Z_ORDER[p // NY]) % NZ) * NY + (y + p % NY) % NY

    def place_of(i, dy):
        return i * NY + (NY - dy) % NY

    def rcopy(src, dst, ss, rs, dev):
        return pltpu.make_async_remote_copy(
            src_ref=src, dst_ref=dst, send_sem=ss, recv_sem=rs, device_id=dev, device_id_type=MESH
        )

    barrier = pltpu.get_barrier_semaphore()
    for i in range(NZ):
        for dy in range(NY):
            if i or dy:
                pl.semaphore_signal(
                    barrier, inc=1, device_id=(2 * expert_of(i, dy) + k, x), device_id_type=MESH
                )
    for dev in (right, left, mate, across):
        pl.semaphore_signal(barrier, inc=1, device_id=dev, device_id_type=MESH)

    w_copies = [
        pltpu.make_async_copy(wg_h.at[0], wg, w_sem.at[0]),
        pltpu.make_async_copy(wu_h.at[0], wu, w_sem.at[1]),
        pltpu.make_async_copy(wd_h.at[0], wd, w_sem.at[2]),
    ]
    for copy in w_copies:
        copy.start()

    lanes = lax.broadcasted_iota(jnp.int32, (TOK, TOK), 1)
    subs = lax.broadcasted_iota(jnp.int32, (TOK, TOK), 0)
    r0 = routes[:, 0:1]
    r1 = routes[:, 1:2]
    a0 = (lanes == r0).astype(F32)
    a1 = (lanes == r1).astype(F32)
    earlier = (lanes < subs).astype(F32).astype(BF16)
    counts = nn(earlier, (a0 + a1).astype(BF16))
    s0 = r0.astype(F32) * MSG + jnp.sum(a0 * counts, axis=1, keepdims=True)
    s1 = r1.astype(F32) * MSG + jnp.sum(a1 * counts, axis=1, keepdims=True)
    eye = lanes == subs
    s0_row = jnp.sum(jnp.where(eye, s0, 0.0), axis=0, keepdims=True)
    s1_row = jnp.sum(jnp.where(eye, s1, 0.0), axis=0, keepdims=True)

    rf = resid[...].astype(F32)
    inv = lax.rsqrt(jnp.mean(rf * rf, axis=-1, keepdims=True) + EPS)
    qcol = m8(x * Q, Q)
    norm_q = (resid[:, pl.ds(qcol, Q)].astype(F32) * inv).astype(BF16)
    og_q = og[:, pl.ds(qcol, Q)].astype(F32)
    w0_q = (rw[:, 0:1] * og_q).astype(BF16)
    w1_q = (rw[:, 1:2] * og_q).astype(BF16)
    data = jnp.concatenate(
        [
            norm_q[:, :256], norm_q[:, 256:],
            w0_q[:, :256], w1_q[:, :256], w0_q[:, 256:], w1_q[:, 256:],
        ],
        axis=0,
    )

    def build(b, carry):
        rows = (lax.broadcasted_iota(jnp.int32, (8 * MSG, TOK), 0) + b * (8 * MSG)).astype(F32)

        def hot(base):
            return (rows == base).astype(F32)

        picks = jnp.concatenate(
            [
                hot(s0_row) + hot(s1_row),
                hot(s0_row + CAP) + hot(s1_row + CAP),
                hot(s0_row + 2 * CAP), hot(s1_row + 2 * CAP),
                hot(s0_row + 3 * CAP), hot(s1_row + 3 * CAP),
            ],
            axis=1,
        ).astype(BF16)
        s_buf[pl.ds(m8(b * 8 * MSG, 8 * MSG), 8 * MSG), :] = nn(picks, data).astype(BF16)
        return carry

    lax.fori_loop(0, GROUPS, build, 0)

    pl.semaphore_wait(barrier, 35)

    def send_rows(i, dy):
        e = expert_of(i, dy)
        p = place_of(i, dy)
        return rcopy(
            s_buf.at[pl.ds(m8(e * MSG), MSG), :],
            r_buf.at[pl.ds(p * MSG, MSG), :],
            pl_s.at[p], pl_r.at[p], (2 * e + k, x),
        )

    own_rows = pltpu.make_async_copy(
        s_buf.at[pl.ds(m8(c * MSG), MSG), :], r_buf.at[pl.ds(0, MSG), :], loc_sem.at[0]
    )
    own_rows.start()
    for i in range(NZ):
        for dy in range(NY):
            if i or dy:
                send_rows(i, dy).start()
    own_rows.wait()

    def col(off):
        return m8(((x + off) % NX) * Q, Q)

    def xa_at(core, g, off, kind=None):
        rows = pl.ds(m8(core * HALF + g * GROW, 16), GROW)
        if kind is None:
            return xa.at[:, rows, pl.ds(col(off), Q)]
        return xa.at[kind, rows, pl.ds(col(off), Q)]

    def x_copy(n, g):
        block, dev = (
            (xa_at(k, g, 0), right),
            (xa_at(k, g, 0), left),
            (xa_at(k, g, 0), mate),
            (xa_at(k, g, 3, 0), right),
            (xa_at(k, g, 1, 1), left),
            (xa_at(k, g, 3), mate),
            (xa_at(k, g, 1), mate),
            (xa_at(k, g, 2), mate),
        )[n]
        return rcopy(block, block, xs.at[n, g], xr.at[n, g], dev)

    def x_wait(n, g):
        block = (
            xa_at(k, g, 3),
            xa_at(k, g, 1),
            xa_at(1 - k, g, 0),
            xa_at(k, g, 2, 0),
            xa_at(k, g, 2, 1),
            xa_at(1 - k, g, 3),
            xa_at(1 - k, g, 1),
            xa_at(1 - k, g, 2),
        )[n]
        rcopy(block, block, xs.at[n, g], xr.at[n, g], mate).wait_recv()

    def plane_wait(buf, rows, sem_s, sem_r, p):
        block = buf.at[pl.ds(m8(p * rows), rows), :]
        rcopy(block, block, sem_s.at[p], sem_r.at[p], mate).wait_recv()

    def stage_in(g):
        def one(j, carry):
            p = g * 8 + j

            @pl.when(p > 0)
            def _():
                plane_wait(r_buf, MSG, pl_s, pl_r, p)

            return carry

        lax.fori_loop(0, 8, one, 0)
        got = nn(perm[...], r_buf[pl.ds(m8(g * 8 * MSG, 8 * MSG), 8 * MSG), :]).astype(BF16)
        rows = pl.ds(m8(k * HALF + g * GROW, 16), GROW)
        for kind in range(2):
            for part in range(2):
                n = 2 * kind + part
                xa[kind, rows, pl.ds(m8(qcol + part * 256, 256), 256)] = got[n * GROW : (n + 1) * GROW]
        for n in (0, 1, 2):
            x_copy(n, g).start()

    def stage_relay(g):
        x_wait(0, g)
        x_copy(3, g).start()
        x_copy(5, g).start()
        x_wait(1, g)
        x_copy(4, g).start()
        x_copy(6, g).start()

    def stage_far(g):
        x_wait(3, g)
        x_wait(4, g)
        x_copy(7, g).start()

    def both(buf, kind, g):
        return jnp.concatenate(
            [buf[kind, pl.ds(m8(core * HALF + g * GROW, 16), GROW), :] for core in range(2)], axis=0
        )

    def stage_compute(g):
        for n in (2, 5, 6, 7):
            x_wait(n, g)
        rows_n = both(xa, 0, g)
        pre_gate = nn(rows_n, wg[...])
        pre_up = nn(rows_n, wu[...])
        d_hidden = nt(both(xa, 1, g), wd[...])
        sig = jax.nn.sigmoid(pre_gate)
        act = pre_gate * sig
        hid_v = (act * pre_up).astype(BF16)
        dg_v = (d_hidden * pre_up * sig * (1.0 + pre_gate * (1.0 - sig))).astype(BF16)
        du_v = (d_hidden * act).astype(BF16)
        for core in range(2):
            rows = pl.ds(m8(core * HALF + g * GROW, 16), GROW)
            part = slice(core * GROW, (core + 1) * GROW)
            hid[rows, :] = hid_v[part]
            dga[rows, :] = dg_v[part]
            dup[rows, :] = du_v[part]

    def step(t, carry):
        @pl.when(t < GROUPS)
        def _():
            stage_in(t)

        @pl.when((t >= 1) & (t < GROUPS + 1))
        def _():
            stage_relay(t - 1)

        @pl.when((t >= 2) & (t < GROUPS + 2))
        def _():
            stage_far(t - 2)

        @pl.when(t == 3)
        def _():
            for copy in w_copies:
                copy.wait()

        @pl.when(t >= 3)
        def _():
            stage_compute(t - 3)

        return carry

    lax.fori_loop(0, GROUPS + 3, step, 0)

    def partial(o, core):
        rows = pl.ds(m8(core * HALF, 16), HALF)
        feats = pl.ds(col(O_OFF[o]), Q)
        return nt(dga[rows, :], wg[feats, :]) + nt(dup[rows, :], wu[feats, :])

    def mate_copy(o):
        return rcopy(ps.at[o], pr.at[o], q_s.at[o], q_r.at[o], mate)

    def make(o):
        ps[o] = partial(o, 1 - k).astype(BF16)
        mate_copy(o).start()
        po[o] = partial(o, k)

    half = HALF // 2
    e_copies = [
        rcopy(cs.at[0, pl.ds(0, half), :], ra, e_s.at[0], e_r.at[0], right),
        rcopy(cs.at[0, pl.ds(half, half), :], rb, e_s.at[1], e_r.at[1], left),
        rcopy(cs.at[1], rc, e_s.at[2], e_r.at[2], right),
        rcopy(cs.at[2], rd, e_s.at[3], e_r.at[3], left),
    ]
    make(0)
    make(1)
    mate_copy(0).wait_recv()
    cs[0] = (po[0] + pr[0].astype(F32)).astype(BF16)
    e_copies[0].start()
    e_copies[1].start()
    make(2)
    mate_copy(1).wait_recv()
    e_copies[0].wait_recv()
    total = po[1] + pr[1].astype(F32)
    cs[1, :half] = (total[:half] + ra[...].astype(F32)).astype(BF16)
    cs[1, half:] = total[half:].astype(BF16)
    e_copies[2].start()
    mate_copy(2).wait_recv()
    e_copies[1].wait_recv()
    total = po[2] + pr[2].astype(F32)
    cs[2, :half] = total[:half].astype(BF16)
    cs[2, half:] = (total[half:] + rb[...].astype(F32)).astype(BF16)
    e_copies[3].start()
    make(3)
    gdn_copy = pltpu.make_async_copy(gdn, gdn_o.at[0], out_sem.at[0])
    gup_copy = pltpu.make_async_copy(gup, gup_o.at[0], out_sem.at[1])

    def down_step(b, carry):
        cols = pl.ds(m8(b * 512, 512), 512)
        gdn[:, cols] = tn(hid[...], xa[1, :, cols]).astype(BF16)
        return carry

    def up_step(b, carry):
        cols = pl.ds(m8(b * 512, 512), 512)
        gup[cols, :] = tn(xa[0, :, cols], dup[...]).astype(BF16)
        return carry

    lax.fori_loop(0, 4, down_step, 0)
    gdn_copy.start()
    mate_copy(3).wait_recv()
    e_copies[2].wait_recv()
    e_copies[3].wait_recv()
    cs[3] = (po[3] + pr[3].astype(F32) + rc[...].astype(F32) + rd[...].astype(F32)).astype(BF16)

    def back_copy(p):
        src = source_of(p)
        return rcopy(
            rt.at[pl.ds(p * MSG, MSG), :],
            bk.at[pl.ds(m8(c * MSG), MSG), :],
            rt_s.at[p], rt_r.at[p], (2 * src + k, x),
        )

    for g in range(GROUPS):
        mine = cs[3, g * GROW : (g + 1) * GROW, :]
        stacked = jnp.concatenate([mine[:, j * 128 : (j + 1) * 128] for j in range(4)], axis=0)
        rt[g * 8 * MSG : (g + 1) * 8 * MSG, :] = nn(perm_t[...], stacked).astype(BF16)
        for j in range(8):
            p = g * 8 + j
            if p:
                back_copy(p).start()
    own_back = pltpu.make_async_copy(
        rt.at[pl.ds(0, MSG), :], bk.at[pl.ds(m8(c * MSG), MSG), :], loc_sem.at[1]
    )
    own_back.start()
    lax.fori_loop(0, 4, up_step, 0)
    gup_copy.start()
    own_back.wait()

    def back_wait(p, carry):
        block = bk.at[pl.ds(m8(p * MSG), MSG), :]
        rcopy(block, block, rt_s.at[p], rt_r.at[p], mate).wait_recv()
        return carry

    lax.fori_loop(1, CHIPS, back_wait, 0)

    cols = lax.broadcasted_iota(jnp.int32, (TOK, CHIPS * MSG), 1).astype(F32)
    back = bk[pl.ds(0, CHIPS * MSG), :]
    for j in range(4):
        hot = ((cols == s0 + j * CAP) | (cols == s1 + j * CAP)).astype(F32).astype(BF16)
        dn[:, pl.ds(m8(qcol + j * 128, 128), 128)] = nn(hot, back).astype(BF16)

    def dn_at(off, rows=None):
        return dn.at[pl.ds(0, TOK) if rows is None else pl.ds(rows, TOK // 2), pl.ds(col(off), Q)]

    def dn_copy(n):
        block, dev = (
            (dn_at(0), right), (dn_at(0), left), (dn_at(3, 0), right), (dn_at(1, TOK // 2), left)
        )[n]
        return rcopy(block, block, dn_s.at[n], dn_r.at[n], dev)

    def dn_wait(n):
        block = (dn_at(3), dn_at(1), dn_at(2, 0), dn_at(2, TOK // 2))[n]
        rcopy(block, block, dn_s.at[n], dn_r.at[n], mate).wait_recv()

    dn_copy(0).start()
    dn_copy(1).start()
    mixed = (ogate[...].astype(F32) * cout[...].astype(F32)).astype(BF16)
    dn_wait(0)
    dn_copy(2).start()
    dn_wait(1)
    dn_copy(3).start()
    dn_wait(2)
    dn_wait(3)

    d_norm = dn[...].astype(F32)
    unit = resid[...].astype(F32) * inv
    row_mean = jnp.mean(unit * d_norm, axis=-1, keepdims=True)
    gr = (og[...].astype(F32) + inv * (d_norm - unit * row_mean)).astype(BF16)
    gr_o[...] = gr

    grad_w = tn(gr, mixed).reshape(CHIPS, 2, 32, C)
    gacc[0] = grad_w[:, 0].reshape(CHIPS * 32, C)
    gacc[1] = grad_w[:, 1].reshape(CHIPS * 32, C)
    gb[...] = gacc[1 - k].astype(BF16)
    gmate = rcopy(gb, gp, t_s.at[0], t_r.at[0], mate)
    gmate.start()

    d_mix = nt(gr, wout[...])
    d_conv = d_mix * ogate[...].astype(F32)
    dcv[...] = d_conv
    to_after = rcopy(dcv.at[pl.ds(TOK - 8, 8), :], hp, t_s.at[1], t_r.at[1], after)
    to_before = rcopy(dcv.at[pl.ds(0, 8), :], hn, t_s.at[2], t_r.at[2], before)
    to_after.start()
    to_before.start()
    gog_o[...] = (d_mix * cout[...].astype(F32)).astype(BF16)

    gmate.wait_recv()
    gs[...] = (gacc[k] + gp[...].astype(F32)).astype(BF16)

    def g_copy(i, dy):
        e = expert_of(i, dy)
        p = place_of(i, dy)
        return rcopy(
            gs.at[pl.ds(m8(e * 32, 32), 32), :],
            g_in.at[pl.ds(p * 32, 32), :],
            g_s.at[p], g_r.at[p], (2 * e + k, x),
        )

    for i in range(NZ - 1, -1, -1):
        for dy in range(NY):
            if i or dy:
                g_copy(i, dy).start()
    own_g = pltpu.make_async_copy(
        gs.at[pl.ds(m8(c * 32, 32), 32), :], g_in.at[pl.ds(0, 32), :], loc_sem.at[2]
    )
    own_g.start()

    to_after.wait_recv()
    to_before.wait_recv()
    row = lax.broadcasted_iota(jnp.int32, (TOK, C), 0)
    next_row = jnp.where(s == 63, 0.0, hn[0:1, :])
    prev_row = jnp.where(s == 0, 0.0, hp[7:8, :])
    nxt = jnp.where(row == TOK - 1, next_row, pltpu.roll(d_conv, TOK - 1, 0))
    prv = jnp.where(row == 0, prev_row, pltpu.roll(d_conv, 1, 0))
    d_inner = taps[0:1, :] * nxt + taps[1:2, :] * d_conv + taps[2:3, :] * prv
    gig_o[...] = (d_inner * cin[...].astype(F32)).astype(BF16)
    gci_o[...] = (d_inner * igate[...].astype(F32)).astype(BF16)

    own_g.wait()

    def g_wait(p, carry):
        plane_wait(g_in, 32, g_s, g_r, p)
        return carry

    lax.fori_loop(1, CHIPS, g_wait, 0)
    gwo_o[...] = jnp.sum(g_in[...].reshape(CHIPS, 32, C).astype(F32), axis=0)

    for i in range(NZ):
        for dy in range(NY):
            if i or dy:
                send_rows(i, dy).wait_send()
                g_copy(i, dy).wait_send()
                back_copy(place_of(i, dy)).wait_send()

    def x_sent(g, carry):
        for n in range(8):
            x_copy(n, g).wait_send()
        return carry

    lax.fori_loop(0, GROUPS, x_sent, 0)
    for o in range(4):
        mate_copy(o).wait_send()
        e_copies[o].wait_send()
        dn_copy(o).wait_send()
    gmate.wait_send()
    to_after.wait_send()
    to_before.wait_send()
    gdn_copy.wait()
    gup_copy.wait()


def per_device(*args):
    place = permutation()
    perm = jnp.asarray(place, BF16)
    perm_t = jnp.asarray(place.T, BF16)
    vmem = pl.BlockSpec(memory_space=pltpu.VMEM)
    hbm = pl.BlockSpec(memory_space=pl.ANY)
    dma = pltpu.SemaphoreType.DMA
    in_specs = [vmem] * 4 + [hbm] * 3 + [vmem] * 8
    out_shape = [
        jax.ShapeDtypeStruct((TOK, D), BF16),
        jax.ShapeDtypeStruct((1, D, H), BF16),
        jax.ShapeDtypeStruct((1, H, D), BF16),
        jax.ShapeDtypeStruct((TOK, C), BF16),
        jax.ShapeDtypeStruct((TOK, C), BF16),
        jax.ShapeDtypeStruct((TOK, C), BF16),
        jax.ShapeDtypeStruct((32, C), F32),
    ]
    out_specs = [vmem, hbm, hbm, vmem, vmem, vmem, vmem]
    slots = CHIPS * MSG
    scratch = [
        pltpu.VMEM((D, H), BF16), pltpu.VMEM((D, H), BF16), pltpu.VMEM((H, D), BF16),
        pltpu.VMEM((slots + 8, 256), BF16), pltpu.VMEM((slots + 8, 256), BF16),
        pltpu.VMEM((2, 2 * HALF, D), BF16),
        pltpu.VMEM((2 * HALF, H), BF16), pltpu.VMEM((2 * HALF, H), BF16), pltpu.VMEM((2 * HALF, H), BF16),
        pltpu.VMEM((4, HALF, Q), BF16), pltpu.VMEM((4, HALF, Q), BF16), pltpu.VMEM((4, HALF, Q), F32),
        pltpu.VMEM((HALF // 2, Q), BF16), pltpu.VMEM((HALF // 2, Q), BF16),
        pltpu.VMEM((HALF, Q), BF16), pltpu.VMEM((HALF, Q), BF16), pltpu.VMEM((4, HALF, Q), BF16),
        pltpu.VMEM((slots + 8, 128), BF16), pltpu.VMEM((slots + 8, 128), BF16),
        pltpu.VMEM((TOK, D), BF16),
        pltpu.VMEM((2, 1024, C), F32), pltpu.VMEM((1024, C), BF16), pltpu.VMEM((1024, C), BF16),
        pltpu.VMEM((1024, C), BF16), pltpu.VMEM((1024, C), BF16),
        pltpu.VMEM((TOK, C), F32), pltpu.VMEM((8, C), F32), pltpu.VMEM((8, C), F32),
        pltpu.VMEM((D, H), BF16), pltpu.VMEM((H, D), BF16),
        dma((3,)), dma((3,)), dma((32,)), dma((32,)), dma((32,)), dma((32,)), dma((32,)), dma((32,)),
        dma((8, 4)), dma((8, 4)), dma((4,)), dma((4,)), dma((4,)), dma((4,)), dma((4,)), dma((4,)),
        dma((3,)), dma((3,)), dma((2,)),
    ]
    return pl.pallas_call(
        kernel,
        out_shape=out_shape,
        in_specs=in_specs,
        out_specs=out_specs,
        scratch_shapes=scratch,
        compiler_params=pltpu.CompilerParams(
            collective_id=0, has_side_effects=True, vmem_limit_bytes=60 * 1024 * 1024
        ),
    )(*args, perm, perm_t)


def solution(mesh):
    in_specs = (
        P("sp", None), P("sp", None), P("sp", None), P("sp", None),
        P("sp", None, "tp"), P("sp", None, "tp"), P("sp", "tp", None),
        P("sp", "tp"), P("sp", "tp"), P("sp", "tp"), P("sp", "tp"),
        P(None, "tp"), P("tp", None),
    )
    out_specs = (
        P("sp", None), P("sp", None, "tp"), P("sp", "tp", None),
        P("sp", "tp"), P("sp", "tp"), P("sp", "tp"), P("sp", "tp"),
    )
    return jax.shard_map(
        per_device, mesh=mesh, in_specs=in_specs, out_specs=out_specs, check_vma=False
    )
```

```python
import jax
import jax.numpy as jnp
import numpy as np
from jax import lax
from jax.experimental import pallas as pl
from jax.experimental.pallas import tpu as pltpu
from jax.sharding import PartitionSpec as P

MESH = pl.DeviceIdType.MESH
EPS = 1e-06
F32 = jnp.float32
BF16 = jnp.bfloat16

D = 2048
H = 512
Q = 512
TOK = 128
CAP = 10
NZ, NY, NX = 8, 4, 4
CHIPS = NZ * NY
MSG = 4 * CAP
GROUPS = 4
GROW = 8 * CAP
HALF = GROUPS * GROW
C = 256
Z_ORDER = (0, 1, 7, 2, 6, 3, 5, 4)
O_OFF = (2, 1, 3, 0)


def permutation():
    place = np.zeros((8 * MSG, 8 * MSG), np.float32)
    for part in range(4):
        for source in range(8):
            for slot in range(CAP):
                place[part * GROW + source * CAP + slot, source * MSG + part * CAP + slot] = 1
    return place


def nt(a, b):
    return lax.dot_general(a, b, (((1,), (1,)), ((), ())), preferred_element_type=F32)


def tn(a, b):
    return lax.dot_general(a, b, (((0,), (0,)), ((), ())), preferred_element_type=F32)


def nn(a, b):
    return jnp.dot(a, b, preferred_element_type=F32)


def m8(value, by=8):
    return pl.multiple_of(value, by)


def kernel(
    og_h, resid_h, routes_h, rw_h, wg_h, wu_h, wd_h, ogate_h, igate_h, cin_h, cout_h, taps_h, wout_h,
    perm_h, perm_t_h,
    gr_o, gup_o, gdn_o, gog_o, gig_o, gci_o, gwo_o,
    og, resid, routes, rw, ogate, igate, cin, cout, taps, wout, perm, perm_t,
    wg, wu, wd, s_buf, r_buf, xa, hid, dga, dup, ps, pr, po, ra, rb, rc, rd, cs, rt, bk, dn,
    gacc, gb, gp, gs, g_in, dcv, hp, hn,
    w_sem, loc_sem, pl_s, pl_r, rt_s, rt_r, g_s, g_r, xs, xr, q_s, q_r, e_s, e_r, dn_s, dn_r, t_s, t_r,
):
    s = lax.axis_index("sp")
    x = lax.axis_index("tp")
    c = s // 2
    k = s % 2
    z = c // NY
    y = c % NY
    right = (s, (x + 1) % NX)
    left = (s, (x + 3) % NX)
    mate = (2 * c + 1 - k, x)
    before = ((s + 63) % 64, x)
    after = ((s + 1) % 64, x)
    across = ((s + 63 + 2 * k) % 64, x)

    def expert_of(i, dy):
        return ((z + NZ - Z_ORDER[i]) % NZ) * NY + (y + dy) % NY

    def place_of(i, dy):
        return i * NY + (NY - dy) % NY

    def rcopy(src, dst, ss, rs, dev):
        return pltpu.make_async_remote_copy(
            src_ref=src, dst_ref=dst, send_sem=ss, recv_sem=rs, device_id=dev, device_id_type=MESH
        )

    barrier = pltpu.get_barrier_semaphore()
    for i in range(NZ):
        for dy in range(NY):
            if i or dy:
                pl.semaphore_signal(
                    barrier, inc=1, device_id=(2 * expert_of(i, dy) + k, x), device_id_type=MESH
                )
    for dev in (right, left, mate, across):
        pl.semaphore_signal(barrier, inc=1, device_id=dev, device_id_type=MESH)

    loads = [
        pltpu.make_async_copy(src, dst, w_sem.at[n])
        for n, (src, dst) in enumerate(
            (
                (routes_h, routes), (rw_h, rw), (resid_h, resid), (og_h, og), (perm_h, perm),
                (wg_h.at[0], wg), (wu_h.at[0], wu), (wd_h.at[0], wd),
                (perm_t_h, perm_t), (ogate_h, ogate), (cout_h, cout), (wout_h, wout),
                (cin_h, cin), (igate_h, igate), (taps_h, taps),
            )
        )
    ]
    for copy in loads[:5]:
        copy.start()

    loads[0].wait()
    loads[1].wait()
    lanes = lax.broadcasted_iota(jnp.int32, (TOK, TOK), 1)
    subs = lax.broadcasted_iota(jnp.int32, (TOK, TOK), 0)
    eye = lanes == subs

    def column(row):
        return jnp.sum(jnp.where(eye, row.astype(F32), 0.0), axis=1, keepdims=True)

    r0 = column(routes[0:1, :])
    r1 = column(routes[1:2, :])
    w0 = column(rw[0:1, :])
    w1 = column(rw[1:2, :])
    a0 = (lanes.astype(F32) == r0).astype(F32)
    a1 = (lanes.astype(F32) == r1).astype(F32)
    earlier = (lanes < subs).astype(F32).astype(BF16)
    counts = nn(earlier, (a0 + a1).astype(BF16))
    s0 = r0 * MSG + jnp.sum(a0 * counts, axis=1, keepdims=True)
    s1 = r1 * MSG + jnp.sum(a1 * counts, axis=1, keepdims=True)
    s0_row = jnp.sum(jnp.where(eye, s0, 0.0), axis=0, keepdims=True)
    s1_row = jnp.sum(jnp.where(eye, s1, 0.0), axis=0, keepdims=True)

    loads[2].wait()
    loads[3].wait()
    rf = resid[...].astype(F32)
    inv = lax.rsqrt(jnp.mean(rf * rf, axis=-1, keepdims=True) + EPS)
    qcol = m8(x * Q, Q)
    norm_q = (resid[:, pl.ds(qcol, Q)].astype(F32) * inv).astype(BF16)
    og_q = og[:, pl.ds(qcol, Q)].astype(F32)
    w0_q = (w0 * og_q).astype(BF16)
    w1_q = (w1 * og_q).astype(BF16)
    data = jnp.concatenate(
        [
            norm_q[:, :256], norm_q[:, 256:],
            w0_q[:, :256], w1_q[:, :256], w0_q[:, 256:], w1_q[:, 256:],
        ],
        axis=0,
    )

    def build(b, carry):
        rows = (lax.broadcasted_iota(jnp.int32, (8 * MSG, TOK), 0) + b * (8 * MSG)).astype(F32)

        def hot(base):
            return (rows == base).astype(F32)

        picks = jnp.concatenate(
            [
                hot(s0_row) + hot(s1_row),
                hot(s0_row + CAP) + hot(s1_row + CAP),
                hot(s0_row + 2 * CAP), hot(s1_row + 2 * CAP),
                hot(s0_row + 3 * CAP), hot(s1_row + 3 * CAP),
            ],
            axis=1,
        ).astype(BF16)
        s_buf[pl.ds(m8(b * 8 * MSG, 8 * MSG), 8 * MSG), :] = nn(picks, data).astype(BF16)
        return carry

    for copy in loads[5:]:
        copy.start()
    lax.fori_loop(0, GROUPS, build, 0)
    loads[4].wait()

    pl.semaphore_wait(barrier, 35)

    def send_rows(i, dy):
        e = expert_of(i, dy)
        p = place_of(i, dy)
        return rcopy(
            s_buf.at[pl.ds(m8(e * MSG), MSG), :],
            r_buf.at[pl.ds(p * MSG, MSG), :],
            pl_s.at[p], pl_r.at[p], (2 * e + k, x),
        )

    own_rows = pltpu.make_async_copy(
        s_buf.at[pl.ds(m8(c * MSG), MSG), :], r_buf.at[pl.ds(0, MSG), :], loc_sem.at[0]
    )
    own_rows.start()
    for i in range(NZ):
        for dy in range(NY):
            if i or dy:
                send_rows(i, dy).start()
    own_rows.wait()

    def col(off):
        return m8(((x + off) % NX) * Q, Q)

    def xa_at(core, g, off, kind=None):
        rows = pl.ds(m8(core * HALF + g * GROW, 16), GROW)
        if kind is None:
            return xa.at[:, rows, pl.ds(col(off), Q)]
        return xa.at[kind, rows, pl.ds(col(off), Q)]

    def x_copy(n, g):
        block, dev = (
            (xa_at(k, g, 0), right),
            (xa_at(k, g, 0), left),
            (xa_at(k, g, 0), mate),
            (xa_at(k, g, 3, 0), right),
            (xa_at(k, g, 1, 1), left),
            (xa_at(k, g, 3), mate),
            (xa_at(k, g, 1), mate),
            (xa_at(k, g, 2), mate),
        )[n]
        return rcopy(block, block, xs.at[n, g], xr.at[n, g], dev)

    def x_wait(n, g):
        block = (
            xa_at(k, g, 3),
            xa_at(k, g, 1),
            xa_at(1 - k, g, 0),
            xa_at(k, g, 2, 0),
            xa_at(k, g, 2, 1),
            xa_at(1 - k, g, 3),
            xa_at(1 - k, g, 1),
            xa_at(1 - k, g, 2),
        )[n]
        rcopy(block, block, xs.at[n, g], xr.at[n, g], mate).wait_recv()

    def plane_wait(buf, rows, sem_s, sem_r, p):
        block = buf.at[pl.ds(m8(p * rows), rows), :]
        rcopy(block, block, sem_s.at[p], sem_r.at[p], mate).wait_recv()

    def stage_in(g):
        def one(j, carry):
            p = g * 8 + j

            @pl.when(p > 0)
            def _():
                plane_wait(r_buf, MSG, pl_s, pl_r, p)

            return carry

        lax.fori_loop(0, 8, one, 0)
        got = nn(perm[...], r_buf[pl.ds(m8(g * 8 * MSG, 8 * MSG), 8 * MSG), :]).astype(BF16)
        rows = pl.ds(m8(k * HALF + g * GROW, 16), GROW)
        for kind in range(2):
            for part in range(2):
                n = 2 * kind + part
                xa[kind, rows, pl.ds(m8(qcol + part * 256, 256), 256)] = got[n * GROW : (n + 1) * GROW]
        for n in (0, 1, 2):
            x_copy(n, g).start()

    def stage_relay(g):
        x_wait(0, g)
        x_copy(3, g).start()
        x_copy(5, g).start()
        x_wait(1, g)
        x_copy(4, g).start()
        x_copy(6, g).start()

    def stage_far(g):
        x_wait(3, g)
        x_wait(4, g)
        x_copy(7, g).start()

    def both(buf, kind, g):
        return jnp.concatenate(
            [buf[kind, pl.ds(m8(core * HALF + g * GROW, 16), GROW), :] for core in range(2)], axis=0
        )

    def stage_compute(g):
        for n in (2, 5, 6, 7):
            x_wait(n, g)
        rows_n = both(xa, 0, g)
        pre_gate = nn(rows_n, wg[...])
        pre_up = nn(rows_n, wu[...])
        d_hidden = nt(both(xa, 1, g), wd[...])
        sig = jax.nn.sigmoid(pre_gate)
        act = pre_gate * sig
        hid_v = (act * pre_up).astype(BF16)
        dg_v = (d_hidden * pre_up * sig * (1.0 + pre_gate * (1.0 - sig))).astype(BF16)
        du_v = (d_hidden * act).astype(BF16)
        for core in range(2):
            rows = pl.ds(m8(core * HALF + g * GROW, 16), GROW)
            part = slice(core * GROW, (core + 1) * GROW)
            hid[rows, :] = hid_v[part]
            dga[rows, :] = dg_v[part]
            dup[rows, :] = du_v[part]

    def mate_copy(g):
        return rcopy(ps.at[g], pr.at[g], q_s.at[g], q_r.at[g], mate)

    def e_copy(n, g):
        src, dst, dev = (
            (cs.at[g, 0, :, pl.ds(0, 256)], ra.at[g], right),
            (cs.at[g, 0, :, pl.ds(256, 256)], rb.at[g], left),
            (cs.at[g, 1], rc.at[g], right),
            (cs.at[g, 2], rd.at[g], left),
        )[n]
        return rcopy(src, dst, e_s.at[n, g], e_r.at[n, g], dev)

    def back_copy(p, source):
        return rcopy(
            rt.at[pl.ds(m8(p * MSG), MSG), :],
            bk.at[pl.ds(m8(c * MSG), MSG), :],
            rt_s.at[p], rt_r.at[p], (2 * source + k, x),
        )

    def source_in(g, j):
        away = (NZ - g) % NZ if j < NY else g + 1
        return ((z + away) % NZ) * NY + (y + j % NY) % NY

    def stage_make(g):
        d_gate = jnp.concatenate(
            [dga[pl.ds(m8(core * HALF + g * GROW, 16), GROW), :] for core in (1 - k, k)], axis=0
        )
        d_up = jnp.concatenate(
            [dup[pl.ds(m8(core * HALF + g * GROW, 16), GROW), :] for core in (1 - k, k)], axis=0
        )
        for o in range(4):
            feats = pl.ds(col(O_OFF[o]), Q)
            part = nt(d_gate, wg[feats, :]) + nt(d_up, wu[feats, :])
            ps[g, o] = part[:GROW].astype(BF16)
            po[g, o] = part[GROW:]
        mate_copy(g).start()

    def stage_first(g):
        mate_copy(g).wait_recv()
        cs[g, 0] = (po[g, 0] + pr[g, 0].astype(F32)).astype(BF16)
        e_copy(0, g).start()
        e_copy(1, g).start()

    def stage_second(g):
        total = po[g, 1] + pr[g, 1].astype(F32)
        e_copy(0, g).wait_recv()
        cs[g, 1, :, 0:256] = (total[:, :256] + ra[g].astype(F32)).astype(BF16)
        cs[g, 1, :, 256:512] = total[:, 256:].astype(BF16)
        e_copy(2, g).start()
        total = po[g, 2] + pr[g, 2].astype(F32)
        e_copy(1, g).wait_recv()
        cs[g, 2, :, 0:256] = total[:, :256].astype(BF16)
        cs[g, 2, :, 256:512] = (total[:, 256:] + rb[g].astype(F32)).astype(BF16)
        e_copy(3, g).start()

    def stage_back(g):
        e_copy(2, g).wait_recv()
        e_copy(3, g).wait_recv()
        mine = (po[g, 3] + pr[g, 3].astype(F32) + rc[g].astype(F32) + rd[g].astype(F32)).astype(BF16)
        stacked = jnp.concatenate([mine[:, j * 128 : (j + 1) * 128] for j in range(4)], axis=0)
        rt[pl.ds(m8(g * 8 * MSG, 8 * MSG), 8 * MSG), :] = nn(perm_t[...], stacked).astype(BF16)
        for j in range(8):
            copy = back_copy(g * 8 + j, source_in(g, j))
            if j:
                copy.start()
            else:
                pl.when(g > 0)(copy.start)

    def down_step(b, carry):
        cols = pl.ds(m8(b * 512, 512), 512)
        gdn_o[0, :, cols] = tn(hid[...], xa[1, :, cols]).astype(BF16)
        return carry

    def up_step(b, carry):
        cols = pl.ds(m8(b * 512, 512), 512)
        gup_o[0, cols, :] = tn(xa[0, :, cols], dup[...]).astype(BF16)
        return carry

    def step(t, carry):
        @pl.when(t < GROUPS)
        def _():
            stage_in(t)

        @pl.when((t >= 1) & (t < GROUPS + 1))
        def _():
            stage_relay(t - 1)

        @pl.when((t >= 2) & (t < GROUPS + 2))
        def _():
            stage_far(t - 2)

        @pl.when(t == 3)
        def _():
            for copy in loads[5:]:
                copy.wait()

        @pl.when((t >= 3) & (t < GROUPS + 3))
        def _():
            stage_compute(t - 3)
            stage_make(t - 3)

        @pl.when((t >= 4) & (t < GROUPS + 4))
        def _():
            stage_first(t - 4)

        @pl.when(t == GROUPS + 4)
        def _():
            lax.fori_loop(0, 4, down_step, 0)

        @pl.when((t >= 5) & (t < GROUPS + 5))
        def _():
            stage_second(t - 5)

        @pl.when(t >= 6)
        def _():
            stage_back(t - 6)

        return carry

    lax.fori_loop(0, GROUPS + 6, step, 0)

    own_back = pltpu.make_async_copy(
        rt.at[pl.ds(0, MSG), :], bk.at[pl.ds(m8(c * MSG), MSG), :], loc_sem.at[1]
    )
    own_back.start()
    lax.fori_loop(0, 4, up_step, 0)
    own_back.wait()

    def back_wait(p, carry):
        block = bk.at[pl.ds(m8(p * MSG), MSG), :]
        rcopy(block, block, rt_s.at[p], rt_r.at[p], mate).wait_recv()
        return carry

    lax.fori_loop(1, CHIPS, back_wait, 0)

    cols = lax.broadcasted_iota(jnp.int32, (TOK, CHIPS * MSG), 1).astype(F32)
    back = bk[pl.ds(0, CHIPS * MSG), :]
    for j in range(4):
        hot = ((cols == s0 + j * CAP) | (cols == s1 + j * CAP)).astype(F32).astype(BF16)
        dn[:, pl.ds(m8(qcol + j * 128, 128), 128)] = nn(hot, back).astype(BF16)

    def dn_at(off, rows=None):
        return dn.at[pl.ds(0, TOK) if rows is None else pl.ds(rows, TOK // 2), pl.ds(col(off), Q)]

    def dn_copy(n):
        block, dev = (
            (dn_at(0), right), (dn_at(0), left), (dn_at(3, 0), right), (dn_at(1, TOK // 2), left)
        )[n]
        return rcopy(block, block, dn_s.at[n], dn_r.at[n], dev)

    def dn_wait(n):
        block = (dn_at(3), dn_at(1), dn_at(2, 0), dn_at(2, TOK // 2))[n]
        rcopy(block, block, dn_s.at[n], dn_r.at[n], mate).wait_recv()

    dn_copy(0).start()
    dn_copy(1).start()
    mixed = (ogate[...].astype(F32) * cout[...].astype(F32)).astype(BF16)
    dn_wait(0)
    dn_copy(2).start()
    dn_wait(1)
    dn_copy(3).start()
    dn_wait(2)
    dn_wait(3)

    d_norm = dn[...].astype(F32)
    unit = resid[...].astype(F32) * inv
    row_mean = jnp.mean(unit * d_norm, axis=-1, keepdims=True)
    gr = (og[...].astype(F32) + inv * (d_norm - unit * row_mean)).astype(BF16)
    gr_o[...] = gr

    grad_w = tn(gr, mixed).reshape(CHIPS, 2, 32, C)
    gacc[0] = grad_w[:, 0].reshape(CHIPS * 32, C)
    gacc[1] = grad_w[:, 1].reshape(CHIPS * 32, C)
    gb[...] = gacc[1 - k].astype(BF16)
    gmate = rcopy(gb, gp, t_s.at[0], t_r.at[0], mate)
    gmate.start()

    d_mix = nt(gr, wout[...])
    d_conv = d_mix * ogate[...].astype(F32)
    dcv[...] = d_conv
    to_after = rcopy(dcv.at[pl.ds(TOK - 8, 8), :], hp, t_s.at[1], t_r.at[1], after)
    to_before = rcopy(dcv.at[pl.ds(0, 8), :], hn, t_s.at[2], t_r.at[2], before)
    to_after.start()
    to_before.start()
    gog_o[...] = (d_mix * cout[...].astype(F32)).astype(BF16)

    gmate.wait_recv()
    gs[...] = (gacc[k] + gp[...].astype(F32)).astype(BF16)

    def g_copy(i, dy):
        e = expert_of(i, dy)
        p = place_of(i, dy)
        return rcopy(
            gs.at[pl.ds(m8(e * 32, 32), 32), :],
            g_in.at[pl.ds(p * 32, 32), :],
            g_s.at[p], g_r.at[p], (2 * e + k, x),
        )

    for i in range(NZ - 1, -1, -1):
        for dy in range(NY):
            if i or dy:
                g_copy(i, dy).start()
    own_g = pltpu.make_async_copy(
        gs.at[pl.ds(m8(c * 32, 32), 32), :], g_in.at[pl.ds(0, 32), :], loc_sem.at[2]
    )
    own_g.start()

    to_after.wait_recv()
    to_before.wait_recv()
    row = lax.broadcasted_iota(jnp.int32, (TOK, C), 0)
    next_row = jnp.where(s == 63, 0.0, hn[0:1, :])
    prev_row = jnp.where(s == 0, 0.0, hp[7:8, :])
    nxt = jnp.where(row == TOK - 1, next_row, pltpu.roll(d_conv, TOK - 1, 0))
    prv = jnp.where(row == 0, prev_row, pltpu.roll(d_conv, 1, 0))
    d_inner = taps[0:1, :] * nxt + taps[1:2, :] * d_conv + taps[2:3, :] * prv
    gig_o[...] = (d_inner * cin[...].astype(F32)).astype(BF16)
    gci_o[...] = (d_inner * igate[...].astype(F32)).astype(BF16)

    own_g.wait()

    def g_wait(p, carry):
        plane_wait(g_in, 32, g_s, g_r, p)
        return carry

    lax.fori_loop(1, CHIPS, g_wait, 0)
    gwo_o[...] = jnp.sum(g_in[...].reshape(CHIPS, 32, C).astype(F32), axis=0)

    for i in range(NZ):
        for dy in range(NY):
            if i or dy:
                send_rows(i, dy).wait_send()
                g_copy(i, dy).wait_send()

    def x_sent(g, carry):
        for n in range(8):
            x_copy(n, g).wait_send()
        mate_copy(g).wait_send()
        for n in range(4):
            e_copy(n, g).wait_send()
        for j in range(8):
            copy = back_copy(g * 8 + j, source_in(g, j))
            if j:
                copy.wait_send()
            else:
                pl.when(g > 0)(copy.wait_send)
        return carry

    lax.fori_loop(0, GROUPS, x_sent, 0)
    for n in range(4):
        dn_copy(n).wait_send()
    gmate.wait_send()
    to_after.wait_send()
    to_before.wait_send()


def finish(*refs):
    ins, outs, sems = refs[:7], refs[7:14], refs[14]
    copies = [pltpu.make_async_copy(a, b, sems.at[n]) for n, (a, b) in enumerate(zip(ins, outs))]
    for copy in copies:
        copy.start()
    for copy in copies:
        copy.wait()


def per_device(*args):
    place = permutation()
    perm = jnp.asarray(place, BF16)
    perm_t = jnp.asarray(place.T, BF16)
    vmem = pl.BlockSpec(memory_space=pltpu.VMEM)
    hbm = pl.BlockSpec(memory_space=pl.ANY)
    dma = pltpu.SemaphoreType.DMA
    shapes = [
        ((TOK, D), BF16), ((1, D, H), BF16), ((1, H, D), BF16),
        ((TOK, C), BF16), ((TOK, C), BF16), ((TOK, C), BF16), ((32, C), F32),
    ]
    slots = CHIPS * MSG
    scratch = [
        pltpu.VMEM((TOK, D), BF16), pltpu.VMEM((TOK, D), BF16),
        pltpu.VMEM((2, TOK), jnp.int32), pltpu.VMEM((2, TOK), F32),
        pltpu.VMEM((TOK, C), BF16), pltpu.VMEM((TOK, C), BF16), pltpu.VMEM((TOK, C), BF16), pltpu.VMEM((TOK, C), BF16),
        pltpu.VMEM((3, C), F32), pltpu.VMEM((C, D), BF16),
        pltpu.VMEM((8 * MSG, 8 * MSG), BF16), pltpu.VMEM((8 * MSG, 8 * MSG), BF16),
        pltpu.VMEM((D, H), BF16), pltpu.VMEM((D, H), BF16), pltpu.VMEM((H, D), BF16),
        pltpu.VMEM((slots + 8, 256), BF16), pltpu.VMEM((slots + 8, 256), BF16),
        pltpu.VMEM((2, 2 * HALF, D), BF16),
        pltpu.VMEM((2 * HALF, H), BF16), pltpu.VMEM((2 * HALF, H), BF16), pltpu.VMEM((2 * HALF, H), BF16),
        pltpu.VMEM((GROUPS, 4, GROW, Q), BF16), pltpu.VMEM((GROUPS, 4, GROW, Q), BF16),
        pltpu.VMEM((GROUPS, 4, GROW, Q), F32),
        pltpu.VMEM((GROUPS, GROW, 256), BF16), pltpu.VMEM((GROUPS, GROW, 256), BF16),
        pltpu.VMEM((GROUPS, GROW, Q), BF16), pltpu.VMEM((GROUPS, GROW, Q), BF16),
        pltpu.VMEM((GROUPS, 4, GROW, Q), BF16),
        pltpu.VMEM((slots + 8, 128), BF16), pltpu.VMEM((slots + 8, 128), BF16),
        pltpu.VMEM((TOK, D), BF16),
        pltpu.VMEM((2, 1024, C), F32), pltpu.VMEM((1024, C), BF16), pltpu.VMEM((1024, C), BF16),
        pltpu.VMEM((1024, C), BF16), pltpu.VMEM((1024, C), BF16),
        pltpu.VMEM((TOK, C), F32), pltpu.VMEM((8, C), F32), pltpu.VMEM((8, C), F32),
        dma((15,)), dma((3,)), dma((32,)), dma((32,)), dma((32,)), dma((32,)), dma((32,)), dma((32,)),
        dma((8, 4)), dma((8, 4)), dma((4,)), dma((4,)), dma((4, 4)), dma((4, 4)), dma((4,)), dma((4,)),
        dma((3,)), dma((3,)),
    ]
    made = pl.pallas_call(
        kernel,
        out_shape=[pltpu.VMEM(*shape) for shape in shapes],
        in_specs=[hbm] * 15,
        out_specs=[vmem] * 7,
        scratch_shapes=scratch,
        compiler_params=pltpu.CompilerParams(
            collective_id=0, has_side_effects=True, vmem_limit_bytes=56 * 1024 * 1024
        ),
    )(*args[:2], args[2].T, args[3].T, *args[4:], perm, perm_t)
    return pl.pallas_call(
        finish,
        out_shape=[jax.ShapeDtypeStruct(*shape) for shape in shapes],
        in_specs=[vmem] * 7,
        out_specs=[hbm] * 7,
        scratch_shapes=[dma((7,))],
        compiler_params=pltpu.CompilerParams(vmem_limit_bytes=1024 * 1024),
    )(*made)


def solution(mesh):
    in_specs = (
        P("sp", None), P("sp", None), P("sp", None), P("sp", None),
        P("sp", None, "tp"), P("sp", None, "tp"), P("sp", "tp", None),
        P("sp", "tp"), P("sp", "tp"), P("sp", "tp"), P("sp", "tp"),
        P(None, "tp"), P("tp", None),
    )
    out_specs = (
        P("sp", None), P("sp", None, "tp"), P("sp", "tp", None),
        P("sp", "tp"), P("sp", "tp"), P("sp", "tp"), P("sp", "tp"),
    )
    return jax.shard_map(
        per_device, mesh=mesh, in_specs=in_specs, out_specs=out_specs, check_vma=False
    )
```

```python
import jax
import jax.numpy as jnp
import numpy as np
from jax import lax
from jax.experimental import pallas as pl
from jax.experimental.pallas import tpu as pltpu
from jax.sharding import PartitionSpec as P

MESH = pl.DeviceIdType.MESH
EPS = 1e-06
F32 = jnp.float32
BF16 = jnp.bfloat16

D = 2048
H = 512
Q = 512
TOK = 128
CAP = 10
NZ, NY, NX = 8, 4, 4
CHIPS = NZ * NY
MSG = 4 * CAP
GROUPS = 4
GROW = 8 * CAP
HALF = GROUPS * GROW
C = 256
Z_ORDER = (0, 1, 7, 2, 6, 3, 5, 4)
W_ORDER = (4, 3, 5, 2, 6, 1, 7, 0)
O_OFF = (2, 1, 3, 0)


def permutation():
    place = np.zeros((8 * MSG, 8 * MSG), np.float32)
    for part in range(4):
        for source in range(8):
            for slot in range(CAP):
                place[part * GROW + source * CAP + slot, source * MSG + part * CAP + slot] = 1
    return place


def nt(a, b):
    return lax.dot_general(a, b, (((1,), (1,)), ((), ())), preferred_element_type=F32)


def tn(a, b):
    return lax.dot_general(a, b, (((0,), (0,)), ((), ())), preferred_element_type=F32)


def nn(a, b):
    return jnp.dot(a, b, preferred_element_type=F32)


def m8(value, by=8):
    return pl.multiple_of(value, by)


def kernel(
    og_h, resid_h, routes_h, rw_h, wg_h, wu_h, wd_h, ogate_h, igate_h, cin_h, cout_h, taps_h, wout_h,
    perm_h, perm_t_h,
    gr_o, gup_o, gdn_o, gog_o, gig_o, gci_o, gwo_o,
    og, resid, routes, rw, ogate, igate, cin, cout, taps, wout, perm, perm_t,
    wg, wu, wd, s_buf, r_buf, xa, hid, dga, dup, ps, pr, po, ra, rb, rc, rd, cs, rt, bk, dn,
    gacc, gb, gp, gs, gy_in, gz_out, gz_in, dcv, halo,
    w_sem, loc_sem, send_sem, pl_r, xr, q_r, e_r, dn_r, g_r, one_r,
):
    s = lax.axis_index("sp")
    x = lax.axis_index("tp")
    c = s // 2
    k = s % 2
    z = c // NY
    y = c % NY
    right = (s, (x + 1) % NX)
    left = (s, (x + 3) % NX)
    mate = (2 * c + 1 - k, x)
    before = ((s + 63) % 64, x)
    after = ((s + 1) % 64, x)
    across = ((s + 63 + 2 * k) % 64, x)

    def expert_of(i, dy):
        return ((z + NZ - Z_ORDER[i]) % NZ) * NY + (y + dy) % NY

    def place_of(i, dy):
        return i * NY + (NY - dy) % NY

    def rcopy(src, dst, ss, rs, dev):
        return pltpu.make_async_remote_copy(
            src_ref=src, dst_ref=dst, send_sem=ss, recv_sem=rs, device_id=dev, device_id_type=MESH
        )

    barrier = pltpu.get_barrier_semaphore()
    for i in range(NZ):
        for dy in range(NY):
            if i or dy:
                pl.semaphore_signal(
                    barrier, inc=1, device_id=(2 * expert_of(i, dy) + k, x), device_id_type=MESH
                )
    for dev in (right, left, mate, across):
        pl.semaphore_signal(barrier, inc=1, device_id=dev, device_id_type=MESH)

    loads = [
        pltpu.make_async_copy(src, dst, w_sem.at[n])
        for n, (src, dst) in enumerate(
            (
                (routes_h, routes), (rw_h, rw), (resid_h, resid), (og_h, og), (perm_h, perm),
                (wg_h.at[0], wg), (wu_h.at[0], wu), (wd_h.at[0], wd),
                (perm_t_h, perm_t), (ogate_h, ogate), (cout_h, cout), (wout_h, wout),
                (cin_h, cin), (igate_h, igate), (taps_h, taps),
            )
        )
    ]
    for copy in loads[:5]:
        copy.start()

    loads[0].wait()
    loads[1].wait()
    lanes = lax.broadcasted_iota(jnp.int32, (TOK, TOK), 1)
    subs = lax.broadcasted_iota(jnp.int32, (TOK, TOK), 0)
    eye = lanes == subs

    def column(row):
        return jnp.sum(jnp.where(eye, row.astype(F32), 0.0), axis=1, keepdims=True)

    r0 = column(routes[0:1, :])
    r1 = column(routes[1:2, :])
    w0 = column(rw[0:1, :])
    w1 = column(rw[1:2, :])
    a0 = (lanes.astype(F32) == r0).astype(F32)
    a1 = (lanes.astype(F32) == r1).astype(F32)
    earlier = (lanes < subs).astype(F32).astype(BF16)
    counts = nn(earlier, (a0 + a1).astype(BF16))
    s0 = r0 * MSG + jnp.sum(a0 * counts, axis=1, keepdims=True)
    s1 = r1 * MSG + jnp.sum(a1 * counts, axis=1, keepdims=True)
    s0_row = jnp.sum(jnp.where(eye, s0, 0.0), axis=0, keepdims=True)
    s1_row = jnp.sum(jnp.where(eye, s1, 0.0), axis=0, keepdims=True)

    loads[2].wait()
    loads[3].wait()
    rf = resid[...].astype(F32)
    inv = lax.rsqrt(jnp.mean(rf * rf, axis=-1, keepdims=True) + EPS)
    qcol = m8(x * Q, Q)
    norm_q = (resid[:, pl.ds(qcol, Q)].astype(F32) * inv).astype(BF16)
    og_q = og[:, pl.ds(qcol, Q)].astype(F32)
    w0_q = (w0 * og_q).astype(BF16)
    w1_q = (w1 * og_q).astype(BF16)
    data = jnp.concatenate(
        [
            norm_q[:, :256], norm_q[:, 256:],
            w0_q[:, :256], w1_q[:, :256], w0_q[:, 256:], w1_q[:, 256:],
        ],
        axis=0,
    )

    def build(b, carry):
        rows = (lax.broadcasted_iota(jnp.int32, (8 * MSG, TOK), 0) + b * (8 * MSG)).astype(F32)

        def hot(base):
            return (rows == base).astype(F32)

        picks = jnp.concatenate(
            [
                hot(s0_row) + hot(s1_row),
                hot(s0_row + CAP) + hot(s1_row + CAP),
                hot(s0_row + 2 * CAP), hot(s1_row + 2 * CAP),
                hot(s0_row + 3 * CAP), hot(s1_row + 3 * CAP),
            ],
            axis=1,
        ).astype(BF16)
        s_buf[pl.ds(m8(b * 8 * MSG, 8 * MSG), 8 * MSG), :] = nn(picks, data).astype(BF16)
        return carry

    for copy in loads[5:]:
        copy.start()
    lax.fori_loop(0, GROUPS, build, 0)
    loads[4].wait()

    pl.semaphore_wait(barrier, 35)

    def send_rows(i, dy):
        e = expert_of(i, dy)
        p = place_of(i, dy)
        return rcopy(
            s_buf.at[pl.ds(m8(e * MSG), MSG), :],
            r_buf.at[pl.ds(p * MSG, MSG), :],
            send_sem.at[0], pl_r.at[i // 2], (2 * e + k, x),
        )

    own_rows = pltpu.make_async_copy(
        s_buf.at[pl.ds(m8(c * MSG), MSG), :], r_buf.at[pl.ds(0, MSG), :], loc_sem.at[0]
    )
    own_rows.start()
    for i in range(NZ):
        for dy in range(NY):
            if i or dy:
                send_rows(i, dy).start()
    own_rows.wait()

    def col(off):
        return m8(((x + off) % NX) * Q, Q)

    def xa_at(core, g, off, kind=None):
        rows = pl.ds(m8(core * HALF + g * GROW, 16), GROW)
        if kind is None:
            return xa.at[:, rows, pl.ds(col(off), Q)]
        return xa.at[kind, rows, pl.ds(col(off), Q)]

    def x_copy(n, g):
        block, dev = (
            (xa_at(k, g, 0), right),
            (xa_at(k, g, 0), left),
            (xa_at(k, g, 0), mate),
            (xa_at(k, g, 3, 0), right),
            (xa_at(k, g, 1, 1), left),
            (xa_at(k, g, 3), mate),
            (xa_at(k, g, 1), mate),
            (xa_at(k, g, 2), mate),
        )[n]
        return rcopy(block, block, send_sem.at[1], xr.at[(0, 1, 3, 2, 2, 3, 3, 3)[n], g], dev)

    def x_wait(n, g):
        block = (
            lambda: xa_at(k, g, 3),
            lambda: xa_at(k, g, 1),
            lambda: xa_at(k, g, 2),
            lambda: xa.at[:, pl.ds(m8((1 - k) * HALF + g * GROW, 16), GROW), :],
        )[n]()
        rcopy(block, block, send_sem.at[1], xr.at[n, g], mate).wait_recv()

    def take(block, sem):
        rcopy(block, block, sem, sem, mate).wait_recv()

    def sent(block, sem):
        rcopy(block, block, sem, sem, mate).wait_send()

    def stage_in(g):
        @pl.when(g == 0)
        def _():
            take(r_buf.at[pl.ds(MSG, 7 * MSG), :], pl_r.at[0])

        @pl.when(g > 0)
        def _():
            take(r_buf.at[pl.ds(m8(g * 8 * MSG, 8 * MSG), 8 * MSG), :], pl_r.at[g])

        got = nn(perm[...], r_buf[pl.ds(m8(g * 8 * MSG, 8 * MSG), 8 * MSG), :]).astype(BF16)
        rows = pl.ds(m8(k * HALF + g * GROW, 16), GROW)
        for kind in range(2):
            for part in range(2):
                n = 2 * kind + part
                xa[kind, rows, pl.ds(m8(qcol + part * 256, 256), 256)] = got[n * GROW : (n + 1) * GROW]
        for n in (0, 1, 2):
            x_copy(n, g).start()

    def stage_relay(g):
        x_wait(0, g)
        x_copy(3, g).start()
        x_copy(5, g).start()
        x_wait(1, g)
        x_copy(4, g).start()
        x_copy(6, g).start()

    def stage_far(g):
        x_wait(2, g)
        x_copy(7, g).start()

    def both(buf, kind, g):
        return jnp.concatenate(
            [buf[kind, pl.ds(m8(core * HALF + g * GROW, 16), GROW), :] for core in range(2)], axis=0
        )

    def stage_compute(g):
        x_wait(3, g)
        rows_n = both(xa, 0, g)
        pre_gate = nn(rows_n, wg[...])
        pre_up = nn(rows_n, wu[...])
        d_hidden = nt(both(xa, 1, g), wd[...])
        sig = jax.nn.sigmoid(pre_gate)
        act = pre_gate * sig
        hid_v = (act * pre_up).astype(BF16)
        dg_v = (d_hidden * pre_up * sig * (1.0 + pre_gate * (1.0 - sig))).astype(BF16)
        du_v = (d_hidden * act).astype(BF16)
        for core in range(2):
            rows = pl.ds(m8(core * HALF + g * GROW, 16), GROW)
            part = slice(core * GROW, (core + 1) * GROW)
            hid[rows, :] = hid_v[part]
            dga[rows, :] = dg_v[part]
            dup[rows, :] = du_v[part]

    def mate_copy(g):
        return rcopy(ps.at[g], pr.at[g], send_sem.at[2], q_r.at[g], mate)

    def e_copy(n, g):
        src, dst, dev = (
            (cs.at[g, 0, :, pl.ds(0, 256)], ra.at[g], right),
            (cs.at[g, 0, :, pl.ds(256, 256)], rb.at[g], left),
            (cs.at[g, 1], rc.at[g], right),
            (cs.at[g, 2], rd.at[g], left),
        )[n]
        return rcopy(src, dst, send_sem.at[3], e_r.at[n // 2, g], dev)

    def back_copy(p, source):
        return rcopy(
            rt.at[pl.ds(m8(p * MSG), MSG), :],
            bk.at[pl.ds(m8(c * MSG), MSG), :],
            send_sem.at[4], one_r.at[0], (2 * source + k, x),
        )

    def source_in(g, j):
        away = (NZ - g) % NZ if j < NY else g + 1
        return ((z + away) % NZ) * NY + (y + j % NY) % NY

    def stage_make(g):
        d_gate = jnp.concatenate(
            [dga[pl.ds(m8(core * HALF + g * GROW, 16), GROW), :] for core in (1 - k, k)], axis=0
        )
        d_up = jnp.concatenate(
            [dup[pl.ds(m8(core * HALF + g * GROW, 16), GROW), :] for core in (1 - k, k)], axis=0
        )
        for o in range(4):
            feats = pl.ds(col(O_OFF[o]), Q)
            part = nt(d_gate, wg[feats, :]) + nt(d_up, wu[feats, :])
            ps[g, o] = part[:GROW].astype(BF16)
            po[g, o] = part[GROW:]
        mate_copy(g).start()

    def stage_first(g):
        mate_copy(g).wait_recv()
        cs[g, 0] = (po[g, 0] + pr[g, 0].astype(F32)).astype(BF16)
        e_copy(0, g).start()
        e_copy(1, g).start()

    def stage_second(g):
        take(cs.at[g, 0], e_r.at[0, g])
        total = po[g, 1] + pr[g, 1].astype(F32)
        cs[g, 1, :, 0:256] = (total[:, :256] + ra[g].astype(F32)).astype(BF16)
        cs[g, 1, :, 256:512] = total[:, 256:].astype(BF16)
        e_copy(2, g).start()
        total = po[g, 2] + pr[g, 2].astype(F32)
        cs[g, 2, :, 0:256] = total[:, :256].astype(BF16)
        cs[g, 2, :, 256:512] = (total[:, 256:] + rb[g].astype(F32)).astype(BF16)
        e_copy(3, g).start()

    def stage_back(g):
        take(cs.at[g, pl.ds(0, 2)], e_r.at[1, g])
        mine = (po[g, 3] + pr[g, 3].astype(F32) + rc[g].astype(F32) + rd[g].astype(F32)).astype(BF16)
        stacked = jnp.concatenate([mine[:, j * 128 : (j + 1) * 128] for j in range(4)], axis=0)
        rt[pl.ds(m8(g * 8 * MSG, 8 * MSG), 8 * MSG), :] = nn(perm_t[...], stacked).astype(BF16)
        for j in range(8):
            copy = back_copy(g * 8 + j, source_in(g, j))
            if j:
                copy.start()
            else:
                pl.when(g > 0)(copy.start)

    def down_step(b, carry):
        cols = pl.ds(m8(b * 512, 512), 512)
        gdn_o[0, :, cols] = tn(hid[...], xa[1, :, cols]).astype(BF16)
        return carry

    def up_step(b, carry):
        cols = pl.ds(m8(b * 512, 512), 512)
        gup_o[0, cols, :] = tn(xa[0, :, cols], dup[...]).astype(BF16)
        return carry

    def step(t, carry):
        @pl.when(t < GROUPS)
        def _():
            stage_in(t)

        @pl.when((t >= 1) & (t < GROUPS + 1))
        def _():
            stage_relay(t - 1)

        @pl.when(t == 3)
        def _():
            for copy in loads[5:]:
                copy.wait()

        @pl.when((t >= 3) & (t < GROUPS + 3))
        def _():
            stage_compute(t - 3)
            stage_make(t - 3)

        @pl.when((t >= 2) & (t < GROUPS + 2))
        def _():
            stage_far(t - 2)

        @pl.when((t >= 4) & (t < GROUPS + 4))
        def _():
            stage_first(t - 4)

        @pl.when((t >= 5) & (t < GROUPS + 5))
        def _():
            stage_second(t - 5)

        @pl.when(t >= 6)
        def _():
            stage_back(t - 6)

        return carry

    lax.fori_loop(0, GROUPS + 6, step, 0)

    own_back = pltpu.make_async_copy(
        rt.at[pl.ds(0, MSG), :], bk.at[pl.ds(m8(c * MSG), MSG), :], loc_sem.at[1]
    )
    own_back.start()
    lax.fori_loop(0, 4, up_step, 0)
    own_back.wait()

    take(bk.at[pl.ds(0, (CHIPS - 1) * MSG), :], one_r.at[0])
    cols = lax.broadcasted_iota(jnp.int32, (TOK, CHIPS * MSG), 1).astype(F32)
    back = bk[pl.ds(0, CHIPS * MSG), :]

    def dn_at(off, h, rows=None):
        return dn.at[
            pl.ds(0, TOK) if rows is None else pl.ds(rows, TOK // 2),
            pl.ds(m8(((x + off) % NX) * Q + h * 256, 256), 256),
        ]

    def dn_copy(n, h):
        block, dev = (
            lambda: (dn_at(0, h), right),
            lambda: (dn_at(0, h), left),
            lambda: (dn_at(3, h, 0), right),
            lambda: (dn_at(1, h, TOK // 2), left),
        )[n]()
        return rcopy(block, block, send_sem.at[5], dn_r.at[(0, 2, 4, 4)[n] + (h if n < 2 else 0)], dev)

    for h in range(2):
        for j in (2 * h, 2 * h + 1):
            hot = ((cols == s0 + j * CAP) | (cols == s1 + j * CAP)).astype(F32).astype(BF16)
            dn[:, pl.ds(m8(qcol + j * 128, 128), 128)] = nn(hot, back).astype(BF16)
        dn_copy(0, h).start()
        dn_copy(1, h).start()
    mixed = (ogate[...].astype(F32) * cout[...].astype(F32)).astype(BF16)
    for h in range(2):
        take(dn_at(3, h), dn_r.at[h])
        dn_copy(2, h).start()
        take(dn_at(1, h), dn_r.at[2 + h])
        dn_copy(3, h).start()
    take(dn.at[:, pl.ds(col(2), Q)], dn_r.at[4])

    d_norm = dn[...].astype(F32)
    unit = resid[...].astype(F32) * inv
    row_mean = jnp.mean(unit * d_norm, axis=-1, keepdims=True)
    gr = (og[...].astype(F32) + inv * (d_norm - unit * row_mean)).astype(BF16)
    gr_o[...] = gr

    grad_w = tn(gr, mixed).reshape(CHIPS, 2, 32, C)
    gacc[0] = grad_w[:, 0].reshape(CHIPS * 32, C)
    gacc[1] = grad_w[:, 1].reshape(CHIPS * 32, C)
    gb[...] = gacc[1 - k].astype(BF16)
    gmate = rcopy(gb, gp, send_sem.at[6], one_r.at[1], mate)
    gmate.start()

    d_mix = nt(gr, wout[...])
    d_conv = d_mix * ogate[...].astype(F32)
    dcv[...] = d_conv
    to_after = rcopy(
        dcv.at[pl.ds(TOK - 8, 8), :], halo.at[pl.ds(0, 8), :], send_sem.at[7], one_r.at[2], after
    )
    to_before = rcopy(
        dcv.at[pl.ds(0, 8), :], halo.at[pl.ds(8, 8), :], send_sem.at[7], one_r.at[2], before
    )
    to_after.start()
    to_before.start()
    gog_o[...] = (d_mix * cout[...].astype(F32)).astype(BF16)

    gmate.wait_recv()
    gs[...] = (gacc[k] + gp[...].astype(F32)).astype(BF16)

    def gs_block(n, dy):
        return pl.ds(m8((((z + W_ORDER[n]) % NZ) * NY + (y + dy) % NY) * 32, 32), 32)

    for h in range(2):
        for n in range(4 * h, 4 * h + 4):
            for dy in range(1, NY):
                rcopy(
                    gs.at[gs_block(n, dy), :],
                    gy_in.at[pl.ds(((dy - 1) * NZ + n) * 32, 32), :],
                    send_sem.at[8], g_r.at[h], (2 * (z * NY + (y + dy) % NY) + k, x),
                ).start()

    lax.fori_loop(0, 4, down_step, 0)

    for h in range(2):
        take(gy_in.at[pl.ds(0, 384), :], g_r.at[h])
        near = jnp.concatenate([gs[gs_block(n, 0), :] for n in range(4 * h, 4 * h + 4)], axis=0)
        total = near.astype(F32)
        for d in range(NY - 1):
            total = total + gy_in[d * 256 + h * 128 : d * 256 + (h + 1) * 128, :].astype(F32)
        gz_out[h * 128 : (h + 1) * 128, :] = total.astype(BF16)
        for n in range(4 * h, 4 * h + 4):
            if W_ORDER[n]:
                rcopy(
                    gz_out.at[pl.ds(n * 32, 32), :], gz_in.at[pl.ds(n * 32, 32), :],
                    send_sem.at[9], g_r.at[2],
                    (2 * (((z + W_ORDER[n]) % NZ) * NY + y) + k, x),
                ).start()
    own_sum = total[96:128]

    take(halo, one_r.at[2])
    row = lax.broadcasted_iota(jnp.int32, (TOK, C), 0)
    next_row = jnp.where(s == 63, 0.0, halo[8:9, :])
    prev_row = jnp.where(s == 0, 0.0, halo[7:8, :])
    nxt = jnp.where(row == TOK - 1, next_row, pltpu.roll(d_conv, TOK - 1, 0))
    prv = jnp.where(row == 0, prev_row, pltpu.roll(d_conv, 1, 0))
    d_inner = taps[0:1, :] * nxt + taps[1:2, :] * d_conv + taps[2:3, :] * prv
    gig_o[...] = (d_inner * cin[...].astype(F32)).astype(BF16)
    gci_o[...] = (d_inner * igate[...].astype(F32)).astype(BF16)

    take(gz_in.at[pl.ds(0, 224), :], g_r.at[2])
    gwo_o[...] = own_sum + jnp.sum(gz_in[0:224, :].reshape(7, 32, C).astype(F32), axis=0)

    sent(s_buf.at[pl.ds(0, (CHIPS - 1) * MSG), :], send_sem.at[0])
    sent(xa.at[:, :, pl.ds(0, 1792)], send_sem.at[1])
    sent(ps, send_sem.at[2])
    sent(cs.at[:, pl.ds(0, 3)], send_sem.at[3])
    sent(rt.at[pl.ds(0, (CHIPS - 1) * MSG), :], send_sem.at[4])
    sent(dn.at[:, pl.ds(0, 1536)], send_sem.at[5])
    sent(gb, send_sem.at[6])
    sent(halo, send_sem.at[7])
    sent(gy_in, send_sem.at[8])
    sent(gz_in.at[pl.ds(0, 224), :], send_sem.at[9])


def finish(*refs):
    ins, outs, sems = refs[:7], refs[7:14], refs[14]
    copies = [pltpu.make_async_copy(a, b, sems.at[n]) for n, (a, b) in enumerate(zip(ins, outs))]
    for copy in copies:
        copy.start()
    for copy in copies:
        copy.wait()


def per_device(*args):
    place = permutation()
    perm = jnp.asarray(place, BF16)
    perm_t = jnp.asarray(place.T, BF16)
    vmem = pl.BlockSpec(memory_space=pltpu.VMEM)
    hbm = pl.BlockSpec(memory_space=pl.ANY)
    dma = pltpu.SemaphoreType.DMA
    shapes = [
        ((TOK, D), BF16), ((1, D, H), BF16), ((1, H, D), BF16),
        ((TOK, C), BF16), ((TOK, C), BF16), ((TOK, C), BF16), ((32, C), F32),
    ]
    slots = CHIPS * MSG
    scratch = [
        pltpu.VMEM((TOK, D), BF16), pltpu.VMEM((TOK, D), BF16),
        pltpu.VMEM((2, TOK), jnp.int32), pltpu.VMEM((2, TOK), F32),
        pltpu.VMEM((TOK, C), BF16), pltpu.VMEM((TOK, C), BF16), pltpu.VMEM((TOK, C), BF16), pltpu.VMEM((TOK, C), BF16),
        pltpu.VMEM((3, C), F32), pltpu.VMEM((C, D), BF16),
        pltpu.VMEM((8 * MSG, 8 * MSG), BF16), pltpu.VMEM((8 * MSG, 8 * MSG), BF16),
        pltpu.VMEM((D, H), BF16), pltpu.VMEM((D, H), BF16), pltpu.VMEM((H, D), BF16),
        pltpu.VMEM((slots + 8, 256), BF16), pltpu.VMEM((slots + 8, 256), BF16),
        pltpu.VMEM((2, 2 * HALF, D), BF16),
        pltpu.VMEM((2 * HALF, H), BF16), pltpu.VMEM((2 * HALF, H), BF16), pltpu.VMEM((2 * HALF, H), BF16),
        pltpu.VMEM((GROUPS, 4, GROW, Q), BF16), pltpu.VMEM((GROUPS, 4, GROW, Q), BF16),
        pltpu.VMEM((GROUPS, 4, GROW, Q), F32),
        pltpu.VMEM((GROUPS, GROW, 256), BF16), pltpu.VMEM((GROUPS, GROW, 256), BF16),
        pltpu.VMEM((GROUPS, GROW, Q), BF16), pltpu.VMEM((GROUPS, GROW, Q), BF16),
        pltpu.VMEM((GROUPS, 4, GROW, Q), BF16),
        pltpu.VMEM((slots + 8, 128), BF16), pltpu.VMEM((slots + 8, 128), BF16),
        pltpu.VMEM((TOK, D), BF16),
        pltpu.VMEM((2, 1024, C), F32), pltpu.VMEM((1024, C), BF16), pltpu.VMEM((1024, C), BF16),
        pltpu.VMEM((1024, C), BF16), pltpu.VMEM((768, C), BF16), pltpu.VMEM((256, C), BF16), pltpu.VMEM((256, C), BF16),
        pltpu.VMEM((TOK, C), F32), pltpu.VMEM((16, C), F32),
        dma((15,)), dma((2,)), dma((10,)), dma((4,)), dma((4, 4)), dma((4,)), dma((2, 4)), dma((5,)), dma((3,)), dma((3,)),
    ]
    made = pl.pallas_call(
        kernel,
        out_shape=[pltpu.VMEM(*shape) for shape in shapes],
        in_specs=[hbm] * 15,
        out_specs=[vmem] * 7,
        scratch_shapes=scratch,
        compiler_params=pltpu.CompilerParams(
            collective_id=0, has_side_effects=True, vmem_limit_bytes=56 * 1024 * 1024
        ),
    )(*args[:2], args[2].T, args[3].T, *args[4:], perm, perm_t)
    return pl.pallas_call(
        finish,
        out_shape=[jax.ShapeDtypeStruct(*shape) for shape in shapes],
        in_specs=[vmem] * 7,
        out_specs=[hbm] * 7,
        scratch_shapes=[dma((7,))],
        compiler_params=pltpu.CompilerParams(vmem_limit_bytes=1024 * 1024),
    )(*made)


def solution(mesh):
    in_specs = (
        P("sp", None), P("sp", None), P("sp", None), P("sp", None),
        P("sp", None, "tp"), P("sp", None, "tp"), P("sp", "tp", None),
        P("sp", "tp"), P("sp", "tp"), P("sp", "tp"), P("sp", "tp"),
        P(None, "tp"), P("tp", None),
    )
    out_specs = (
        P("sp", None), P("sp", None, "tp"), P("sp", "tp", None),
        P("sp", "tp"), P("sp", "tp"), P("sp", "tp"), P("sp", "tp"),
    )
    return jax.shard_map(
        per_device, mesh=mesh, in_specs=in_specs, out_specs=out_specs, check_vma=False
    )
```

```python
import jax
import jax.numpy as jnp
import numpy as np
from jax import lax
from jax.experimental import pallas as pl
from jax.experimental.pallas import tpu as pltpu
from jax.sharding import PartitionSpec as P

MESH = pl.DeviceIdType.MESH
EPS = 1e-06
F32 = jnp.float32
BF16 = jnp.bfloat16

D = 2048
H = 512
Q = 512
TOK = 128
CAP = 10
NZ, NY, NX = 8, 4, 4
CHIPS = NZ * NY
MSG = 4 * CAP
GROUPS = 4
GROW = 8 * CAP
HALF = GROUPS * GROW
C = 256
Z_ORDER = (0, 1, 6, 3, 5, 4, 7, 2)
O_OFF = (2, 1, 3, 0)


def permutation(sources):
    place = np.zeros((sources * MSG, sources * MSG), np.float32)
    for part in range(4):
        for source in range(sources):
            for slot in range(CAP):
                place[(part * sources + source) * CAP + slot, source * MSG + part * CAP + slot] = 1
    return place


def nt(a, b):
    return lax.dot_general(a, b, (((1,), (1,)), ((), ())), preferred_element_type=F32)


def tn(a, b):
    return lax.dot_general(a, b, (((0,), (0,)), ((), ())), preferred_element_type=F32)


def nn(a, b):
    return jnp.dot(a, b, preferred_element_type=F32)


def m8(value, by=8):
    return pl.multiple_of(value, by)


def kernel(
    og_h, resid_h, routes_h, rw_h, wg_h, wu_h, wd_h, ogate_h, igate_h, cin_h, cout_h, taps_h, wout_h,
    perm_h, perm_t_h,
    gr_o, gup_o, gdn_o, gog_o, gig_o, gci_o, gwo_o,
    og, resid, routes, rw, ogate, igate, cin, cout, taps, wout, perm, perm_t,
    wg, wu, wd, s_buf, r_buf, xa, hid, dga, dup, ps, pr, po, ra, rb, rc, rd, cs, rt, bk, dn,
    gacc, gb, gp, gs, gy_in, gz_out, gz_in, dcv, halo, dots,
    w_sem, loc_sem, send_sem, pl_r, xr, q_r, e_r, dn_r, g_r, one_r, gm_r,
):
    s = lax.axis_index("sp")
    x = lax.axis_index("tp")
    c = s // 2
    k = s % 2
    z = c // NY
    y = c % NY
    right = (s, (x + 1) % NX)
    left = (s, (x + 3) % NX)
    far = (s, (x + 2) % NX)
    mate = (2 * c + 1 - k, x)
    before = ((s + 63) % 64, x)
    after = ((s + 1) % 64, x)
    across = ((s + 63 + 2 * k) % 64, x)

    def expert_of(i, dy):
        return ((z + NZ - Z_ORDER[i]) % NZ) * NY + (y + dy) % NY

    def place_of(i, dy):
        return i * NY + (NY - dy) % NY

    def rcopy(src, dst, ss, rs, dev):
        return pltpu.make_async_remote_copy(
            src_ref=src, dst_ref=dst, send_sem=ss, recv_sem=rs, device_id=dev, device_id_type=MESH
        )

    barrier = pltpu.get_barrier_semaphore()
    for i in range(NZ):
        for dy in range(NY):
            if i or dy:
                pl.semaphore_signal(
                    barrier, inc=1, device_id=(2 * expert_of(i, dy) + k, x), device_id_type=MESH
                )
    for dev in (right, left, far, mate, across):
        pl.semaphore_signal(barrier, inc=1, device_id=dev, device_id_type=MESH)

    loads = [
        pltpu.make_async_copy(src, dst, w_sem.at[n])
        for n, (src, dst) in enumerate(
            (
                (routes_h, routes), (rw_h, rw), (resid_h, resid), (og_h, og), (perm_h, perm),
                (wg_h.at[0], wg), (wu_h.at[0], wu), (wd_h.at[0], wd),
                (perm_t_h, perm_t), (ogate_h, ogate), (cout_h, cout), (wout_h, wout),
                (cin_h, cin), (igate_h, igate), (taps_h, taps),
            )
        )
    ]
    for copy in loads[:5]:
        copy.start()

    loads[0].wait()
    loads[1].wait()
    lanes = lax.broadcasted_iota(jnp.int32, (TOK, TOK), 1)
    subs = lax.broadcasted_iota(jnp.int32, (TOK, TOK), 0)
    eye = lanes == subs

    def column(row):
        return jnp.sum(jnp.where(eye, row.astype(F32), 0.0), axis=1, keepdims=True)

    r0 = column(routes[0:1, :])
    r1 = column(routes[1:2, :])
    w0 = column(rw[0:1, :])
    w1 = column(rw[1:2, :])
    a0 = (lanes.astype(F32) == r0).astype(F32)
    a1 = (lanes.astype(F32) == r1).astype(F32)
    earlier = (lanes < subs).astype(F32).astype(BF16)
    counts = nn(earlier, (a0 + a1).astype(BF16))
    s0 = r0 * MSG + jnp.sum(a0 * counts, axis=1, keepdims=True)
    s1 = r1 * MSG + jnp.sum(a1 * counts, axis=1, keepdims=True)
    s0_row = jnp.sum(jnp.where(eye, s0, 0.0), axis=0, keepdims=True)
    s1_row = jnp.sum(jnp.where(eye, s1, 0.0), axis=0, keepdims=True)

    loads[2].wait()
    loads[3].wait()
    rf = resid[...].astype(F32)
    inv = lax.rsqrt(jnp.mean(rf * rf, axis=-1, keepdims=True) + EPS)
    qcol = m8(x * Q, Q)
    norm_q = (resid[:, pl.ds(qcol, Q)].astype(F32) * inv).astype(BF16)
    og_q = og[:, pl.ds(qcol, Q)].astype(F32)
    w0_q = (w0 * og_q).astype(BF16)
    w1_q = (w1 * og_q).astype(BF16)
    data = jnp.concatenate(
        [
            norm_q[:, :256], norm_q[:, 256:],
            w0_q[:, :256], w1_q[:, :256], w0_q[:, 256:], w1_q[:, 256:],
        ],
        axis=0,
    )

    def build(b, carry):
        rows = (lax.broadcasted_iota(jnp.int32, (8 * MSG, TOK), 0) + b * (8 * MSG)).astype(F32)

        def hot(base):
            return (rows == base).astype(F32)

        picks = jnp.concatenate(
            [
                hot(s0_row) + hot(s1_row),
                hot(s0_row + CAP) + hot(s1_row + CAP),
                hot(s0_row + 2 * CAP), hot(s1_row + 2 * CAP),
                hot(s0_row + 3 * CAP), hot(s1_row + 3 * CAP),
            ],
            axis=1,
        ).astype(BF16)
        s_buf[pl.ds(m8(b * 8 * MSG, 8 * MSG), 8 * MSG), :] = nn(picks, data).astype(BF16)
        return carry

    for copy in loads[5:]:
        copy.start()
    lax.fori_loop(0, GROUPS, build, 0)
    loads[4].wait()

    pl.semaphore_wait(barrier, 36)

    def send_rows(i, dy):
        e = expert_of(i, dy)
        p = place_of(i, dy)
        return rcopy(
            s_buf.at[pl.ds(m8(e * MSG), MSG), :],
            r_buf.at[pl.ds(p * MSG, MSG), :],
            send_sem.at[0], pl_r.at[i], (2 * e + k, x),
        )

    own_rows = pltpu.make_async_copy(
        s_buf.at[pl.ds(m8(c * MSG), MSG), :], r_buf.at[pl.ds(0, MSG), :], loc_sem.at[0]
    )
    own_rows.start()
    for i in range(NZ):
        for dy in range(NY):
            if i or dy:
                send_rows(i, dy).start()
    own_rows.wait()

    def col(off):
        return m8(((x + off) % NX) * Q, Q)

    def xa_at(core, g, off, kind=None):
        rows = pl.ds(m8(core * HALF + g * GROW, 16), GROW)
        if kind is None:
            return xa.at[:, rows, pl.ds(col(off), Q)]
        return xa.at[kind, rows, pl.ds(col(off), Q)]

    def own_copy(n, g, half):
        block = xa.at[
            :, pl.ds(m8(k * HALF + g * GROW + half * (GROW // 2)), GROW // 2), pl.ds(qcol, Q)
        ]
        return rcopy(block, block, send_sem.at[1], xr.at[(0, 1, 3)[n], g], (right, left, mate)[n])

    def x_copy(n, g):
        block, dev = {
            3: lambda: (xa_at(k, g, 3, 0), right),
            4: lambda: (xa_at(k, g, 1, 1), left),
            5: lambda: (xa_at(k, g, 3), mate),
            6: lambda: (xa_at(k, g, 1), mate),
            7: lambda: (xa_at(k, g, 2), mate),
        }[n]()
        return rcopy(block, block, send_sem.at[1], xr.at[2 if n < 5 else 3, g], dev)

    def x_wait(n, g):
        block = (
            lambda: xa_at(k, g, 3),
            lambda: xa_at(k, g, 1),
            lambda: xa_at(k, g, 2),
            lambda: xa.at[:, pl.ds(m8((1 - k) * HALF + g * GROW, 16), GROW), :],
        )[n]()
        rcopy(block, block, send_sem.at[1], xr.at[n, g], mate).wait_recv()

    def take(block, sem):
        rcopy(block, block, sem, sem, mate).wait_recv()

    def sent(block, sem):
        rcopy(block, block, sem, sem, mate).wait_send()

    def stage_in(g):
        for half in range(2):
            base = (2 * g + half) * NY * MSG
            if half:
                take(r_buf.at[pl.ds(m8(base, NY * MSG), NY * MSG), :], pl_r.at[2 * g + 1])
            else:

                @pl.when(g == 0)
                def _():
                    take(r_buf.at[pl.ds(MSG, 3 * MSG), :], pl_r.at[0])

                @pl.when(g > 0)
                def _():
                    take(r_buf.at[pl.ds(m8(base, NY * MSG), NY * MSG), :], pl_r.at[2 * g])

            got = nn(perm[...], r_buf[pl.ds(m8(base, NY * MSG), NY * MSG), :]).astype(BF16)
            rows = pl.ds(m8(k * HALF + g * GROW + half * (GROW // 2)), GROW // 2)
            for kind in range(2):
                for part in range(2):
                    n = 2 * kind + part
                    xa[kind, rows, pl.ds(m8(qcol + part * 256, 256), 256)] = got[n * MSG : (n + 1) * MSG]
            for n in range(3):
                own_copy(n, g, half).start()

    def stage_relay(g):
        x_wait(0, g)
        x_copy(3, g).start()
        x_copy(5, g).start()
        x_wait(1, g)
        x_copy(4, g).start()
        x_copy(6, g).start()

    def stage_far(g):
        x_wait(2, g)
        x_copy(7, g).start()

    def both(buf, kind, g):
        return jnp.concatenate(
            [buf[kind, pl.ds(m8(core * HALF + g * GROW, 16), GROW), :] for core in range(2)], axis=0
        )

    def stage_compute(g):
        x_wait(3, g)
        rows_n = both(xa, 0, g)
        pre_gate = nn(rows_n, wg[...])
        pre_up = nn(rows_n, wu[...])
        d_hidden = nt(both(xa, 1, g), wd[...])
        sig = jax.nn.sigmoid(pre_gate)
        act = pre_gate * sig
        hid_v = (act * pre_up).astype(BF16)
        dg_v = (d_hidden * pre_up * sig * (1.0 + pre_gate * (1.0 - sig))).astype(BF16)
        du_v = (d_hidden * act).astype(BF16)
        for core in range(2):
            rows = pl.ds(m8(core * HALF + g * GROW, 16), GROW)
            part = slice(core * GROW, (core + 1) * GROW)
            hid[rows, :] = hid_v[part]
            dga[rows, :] = dg_v[part]
            dup[rows, :] = du_v[part]

    def mate_copy(g):
        return rcopy(ps.at[g], pr.at[g], send_sem.at[2], q_r.at[g], mate)

    def e_copy(n, g):
        src, dst, dev = (
            (cs.at[g, 0, :, pl.ds(0, 256)], ra.at[g], right),
            (cs.at[g, 0, :, pl.ds(256, 256)], rb.at[g], left),
            (cs.at[g, 1], rc.at[g], right),
            (cs.at[g, 2], rd.at[g], left),
        )[n]
        return rcopy(src, dst, send_sem.at[3], e_r.at[n // 2, g], dev)

    def back_copy(p, source):
        return rcopy(
            rt.at[pl.ds(m8(p * MSG), MSG), :],
            bk.at[pl.ds(m8(c * MSG), MSG), :],
            send_sem.at[4], one_r.at[0], (2 * source + k, x),
        )

    def source_in(g, j):
        away = 0
        for n in range(1 if j < NY else 0, GROUPS):
            away = away + Z_ORDER[2 * n + j // NY] * (1 - ((g - n) * (g - n) + 8) // 9)
        return ((z + away) % NZ) * NY + (y + j % NY) % NY

    def stage_make(g):
        d_gate = jnp.concatenate(
            [dga[pl.ds(m8(core * HALF + g * GROW, 16), GROW), :] for core in (1 - k, k)], axis=0
        )
        d_up = jnp.concatenate(
            [dup[pl.ds(m8(core * HALF + g * GROW, 16), GROW), :] for core in (1 - k, k)], axis=0
        )
        for o in range(4):
            feats = pl.ds(col(O_OFF[o]), Q)
            part = nt(d_gate, wg[feats, :]) + nt(d_up, wu[feats, :])
            ps[g, o] = part[:GROW].astype(BF16)
            po[g, o] = part[GROW:]
        mate_copy(g).start()

    def stage_first(g):
        mate_copy(g).wait_recv()
        cs[g, 0] = (po[g, 0] + pr[g, 0].astype(F32)).astype(BF16)
        e_copy(0, g).start()
        e_copy(1, g).start()

    def stage_second(g):
        take(cs.at[g, 0], e_r.at[0, g])
        total = po[g, 1] + pr[g, 1].astype(F32)
        cs[g, 1, :, 0:256] = (total[:, :256] + ra[g].astype(F32)).astype(BF16)
        cs[g, 1, :, 256:512] = total[:, 256:].astype(BF16)
        e_copy(2, g).start()
        total = po[g, 2] + pr[g, 2].astype(F32)
        cs[g, 2, :, 0:256] = total[:, :256].astype(BF16)
        cs[g, 2, :, 256:512] = (total[:, 256:] + rb[g].astype(F32)).astype(BF16)
        e_copy(3, g).start()

    def stage_back(g):
        take(cs.at[g, pl.ds(0, 2)], e_r.at[1, g])
        mine = (po[g, 3] + pr[g, 3].astype(F32) + rc[g].astype(F32) + rd[g].astype(F32)).astype(BF16)
        stacked = jnp.concatenate([mine[:, j * 128 : (j + 1) * 128] for j in range(4)], axis=0)
        rt[pl.ds(m8(g * 8 * MSG, 8 * MSG), 8 * MSG), :] = nn(perm_t[...], stacked).astype(BF16)
        for j in range(8):
            copy = back_copy(g * 8 + j, source_in(g, j))
            if j:
                copy.start()
            else:
                pl.when(g > 0)(copy.start)

    def down_step(b, carry):
        cols = pl.ds(m8(b * 512, 512), 512)
        gdn_o[0, :, cols] = tn(hid[...], xa[1, 0 : 2 * HALF, cols]).astype(BF16)
        return carry

    def up_step(b, carry):
        cols = pl.ds(m8(b * 512, 512), 512)
        gup_o[0, cols, :] = tn(xa[0, 0 : 2 * HALF, cols], dup[...]).astype(BF16)
        return carry

    def step(t, carry):
        @pl.when(t < GROUPS)
        def _():
            stage_in(t)

        @pl.when((t >= 1) & (t < GROUPS + 1))
        def _():
            stage_relay(t - 1)

        @pl.when(t == 3)
        def _():
            for copy in loads[5:]:
                copy.wait()

        @pl.when((t == 2) | ((t >= 4) & (t < GROUPS + 2)))
        def _():
            stage_far(t - 2)

        @pl.when((t >= 3) & (t < GROUPS + 3))
        def _():
            stage_compute(t - 3)
            stage_make(t - 3)

        @pl.when(t == 3)
        def _():
            stage_far(t - 2)

        @pl.when((t >= 4) & (t < GROUPS + 4))
        def _():
            stage_first(t - 4)

        @pl.when((t >= 5) & (t < GROUPS + 5))
        def _():
            stage_second(t - 5)

        @pl.when(t >= 6)
        def _():
            stage_back(t - 6)

        return carry

    lax.fori_loop(0, GROUPS + 6, step, 0)

    own_back = pltpu.make_async_copy(
        rt.at[pl.ds(0, MSG), :], bk.at[pl.ds(m8(c * MSG), MSG), :], loc_sem.at[1]
    )
    own_back.start()
    lax.fori_loop(0, 4, up_step, 0)
    own_back.wait()

    take(bk.at[pl.ds(0, (CHIPS - 1) * MSG), :], one_r.at[0])
    cols = lax.broadcasted_iota(jnp.int32, (TOK, CHIPS * MSG), 1).astype(F32)
    back = bk[pl.ds(0, CHIPS * MSG), :]

    def dn_at(off, h, rows=None):
        return dn.at[
            pl.ds(0, TOK) if rows is None else pl.ds(rows, TOK // 2),
            pl.ds(m8(((x + off) % NX) * Q + h * 256, 256), 256),
        ]

    def dn_copy(n, h):
        block, dev = (
            lambda: (dn_at(0, h), right),
            lambda: (dn_at(0, h), left),
            lambda: (dn_at(3, h, 0), right),
            lambda: (dn_at(1, h, TOK // 2), left),
        )[n]()
        return rcopy(block, block, send_sem.at[5], dn_r.at[(0, 2, 4, 4)[n] + (h if n < 2 else 0)], dev)

    for j in range(4):
        hot = ((cols == s0 + j * CAP) | (cols == s1 + j * CAP)).astype(F32).astype(BF16)
        dn[:, pl.ds(m8(qcol + j * 128, 128), 128)] = nn(hot, back).astype(BF16)

    def unit_of(feats):
        return resid[:, feats].astype(F32) * inv

    own_feats = pl.ds(qcol, Q)
    part = jnp.sum(unit_of(own_feats) * dn[:, own_feats].astype(F32), axis=1, keepdims=True)
    part = jnp.sum(jnp.where(eye, part, 0.0), axis=0, keepdims=True)
    dots[x] = jnp.broadcast_to(part, (8, TOK))
    for dev in (right, left, far):
        rcopy(dots.at[x], dots.at[x], send_sem.at[10], one_r.at[3], dev).start()
    for h in range(2):
        dn_copy(0, h).start()
        dn_copy(1, h).start()
    mixed = (ogate[...].astype(F32) * cout[...].astype(F32)).astype(BF16)
    take(dots.at[pl.ds(0, 3)], one_r.at[3])
    means = (dots[0, 0:1, :] + dots[1, 0:1, :] + dots[2, 0:1, :] + dots[3, 0:1, :]) * (1.0 / D)
    row_mean = jnp.sum(jnp.where(eye, means, 0.0), axis=1, keepdims=True)

    def quarter_rows(off):
        return pl.ds(m8(((x + off) % NX) * 256, 256), 256)

    def quarter(off, chunk):
        feats = pl.ds(col(off), Q)
        rows = quarter_rows(off)
        gr = (
            og[:, feats].astype(F32)
            + inv * (dn[:, feats].astype(F32) - unit_of(feats) * row_mean)
        ).astype(BF16)
        gr_o[:, feats] = gr
        grad_w = tn(gr, mixed).reshape(8, 2, 32, C)
        gacc[0, rows, :] = grad_w[:, 0].reshape(256, C)
        gacc[1, rows, :] = grad_w[:, 1].reshape(256, C)
        gb[rows, :] = gacc[1 - k, rows, :].astype(BF16)
        rcopy(gb.at[rows, :], gp.at[rows, :], send_sem.at[6], gm_r.at[chunk], mate).start()

    def along_y(offs, first, chunk):
        for n, off in enumerate(offs):
            rows = quarter_rows(off)
            gs[rows, :] = (gacc[k, rows, :] + gp[rows, :].astype(F32)).astype(BF16)
            for zz in range(2):
                for dy in range(1, NY):
                    there = (y + dy) % NY
                    block = ((2 * ((x + off) % NX) + zz) * NY + there) * 32
                    rcopy(
                        gs.at[pl.ds(m8(block, 32), 32), :],
                        gy_in.at[pl.ds(((dy - 1) * NZ + first + 2 * n + zz) * 32, 32), :],
                        send_sem.at[8], g_r.at[chunk], (2 * (z * NY + there) + k, x),
                    ).start()

    def along_z(offs, first):
        for n, off in enumerate(offs):
            for zz in range(2):
                there = 2 * ((x + off) % NX) + zz
                slot = (first + 2 * n + zz) * 32
                total = gs[pl.ds(m8((there * NY + y) * 32, 32), 32), :].astype(F32)
                for d in range(NY - 1):
                    total = total + gy_in[d * 256 + slot : d * 256 + slot + 32, :].astype(F32)
                gz_out[slot : slot + 32, :] = total.astype(BF16)

                @pl.when(there == z)
                def _():
                    gz_in[pl.ds(m8(z * 32, 32), 32), :] = gz_out[slot : slot + 32, :]

                @pl.when(there != z)
                def _():
                    rcopy(
                        gz_out.at[pl.ds(slot, 32), :], gz_in.at[pl.ds(m8(z * 32, 32), 32), :],
                        send_sem.at[9], g_r.at[2], (2 * (there * NY + y) + k, x),
                    ).start()

    near = (0, 3, 1)
    quarter(0, 0)
    for h in range(2):
        take(dn_at(3, h), dn_r.at[h])
        dn_copy(2, h).start()
        take(dn_at(1, h), dn_r.at[2 + h])
        dn_copy(3, h).start()
    quarter(3, 0)
    quarter(1, 0)
    take(gp.at[pl.ds(0, 768), :], gm_r.at[0])
    along_y(near, 0, 0)
    take(dn.at[:, pl.ds(col(2), Q)], dn_r.at[4])
    quarter(2, 1)

    d_mix = nt(gr_o[...], wout[...])
    d_conv = d_mix * ogate[...].astype(F32)
    dcv[...] = d_conv
    to_after = rcopy(
        dcv.at[pl.ds(TOK - 8, 8), :], halo.at[pl.ds(0, 8), :], send_sem.at[7], one_r.at[2], after
    )
    to_before = rcopy(
        dcv.at[pl.ds(0, 8), :], halo.at[pl.ds(8, 8), :], send_sem.at[7], one_r.at[2], before
    )
    to_after.start()
    to_before.start()
    gog_o[...] = (d_mix * cout[...].astype(F32)).astype(BF16)

    take(gp.at[pl.ds(0, 256), :], gm_r.at[1])
    along_y((2,), 6, 1)
    take(gy_in.at[pl.ds(0, 576), :], g_r.at[0])
    along_z(near, 0)
    lax.fori_loop(0, 4, down_step, 0)
    take(gy_in.at[pl.ds(0, 192), :], g_r.at[1])
    along_z((2,), 6)

    take(halo, one_r.at[2])
    row = lax.broadcasted_iota(jnp.int32, (TOK, C), 0)
    next_row = jnp.where(s == 63, 0.0, halo[8:9, :])
    prev_row = jnp.where(s == 0, 0.0, halo[7:8, :])
    nxt = jnp.where(row == TOK - 1, next_row, pltpu.roll(d_conv, TOK - 1, 0))
    prv = jnp.where(row == 0, prev_row, pltpu.roll(d_conv, 1, 0))
    d_inner = taps[0:1, :] * nxt + taps[1:2, :] * d_conv + taps[2:3, :] * prv
    gig_o[...] = (d_inner * cin[...].astype(F32)).astype(BF16)
    gci_o[...] = (d_inner * igate[...].astype(F32)).astype(BF16)

    take(gz_in.at[pl.ds(0, 224), :], g_r.at[2])
    gwo_o[...] = jnp.sum(gz_in[...].reshape(NZ, 32, C).astype(F32), axis=0)

    sent(s_buf.at[pl.ds(0, (CHIPS - 1) * MSG), :], send_sem.at[0])
    sent(xa.at[:, pl.ds(0, 2 * HALF), pl.ds(0, 1792)], send_sem.at[1])
    sent(ps, send_sem.at[2])
    sent(cs.at[:, pl.ds(0, 3)], send_sem.at[3])
    sent(rt.at[pl.ds(0, (CHIPS - 1) * MSG), :], send_sem.at[4])
    sent(dn.at[:, pl.ds(0, 1536)], send_sem.at[5])
    sent(gb, send_sem.at[6])
    sent(halo, send_sem.at[7])
    sent(gy_in, send_sem.at[8])
    sent(gz_in.at[pl.ds(0, 224), :], send_sem.at[9])
    sent(dots.at[pl.ds(0, 3)], send_sem.at[10])


def finish(*refs):
    ins, outs, sems = refs[:7], refs[7:14], refs[14]
    copies = [pltpu.make_async_copy(a, b, sems.at[n]) for n, (a, b) in enumerate(zip(ins, outs))]
    for copy in copies:
        copy.start()
    for copy in copies:
        copy.wait()


def per_device(*args):
    perm = jnp.asarray(permutation(NY), BF16)
    perm_t = jnp.asarray(permutation(8).T, BF16)
    vmem = pl.BlockSpec(memory_space=pltpu.VMEM)
    hbm = pl.BlockSpec(memory_space=pl.ANY)
    dma = pltpu.SemaphoreType.DMA
    shapes = [
        ((TOK, D), BF16), ((1, D, H), BF16), ((1, H, D), BF16),
        ((TOK, C), BF16), ((TOK, C), BF16), ((TOK, C), BF16), ((32, C), F32),
    ]
    slots = CHIPS * MSG
    scratch = [
        pltpu.VMEM((TOK, D), BF16), pltpu.VMEM((TOK, D), BF16),
        pltpu.VMEM((2, TOK), jnp.int32), pltpu.VMEM((2, TOK), F32),
        pltpu.VMEM((TOK, C), BF16), pltpu.VMEM((TOK, C), BF16), pltpu.VMEM((TOK, C), BF16), pltpu.VMEM((TOK, C), BF16),
        pltpu.VMEM((3, C), F32), pltpu.VMEM((C, D), BF16),
        pltpu.VMEM((NY * MSG, NY * MSG), BF16), pltpu.VMEM((8 * MSG, 8 * MSG), BF16),
        pltpu.VMEM((D, H), BF16), pltpu.VMEM((D, H), BF16), pltpu.VMEM((H, D), BF16),
        pltpu.VMEM((slots + 8, 256), BF16), pltpu.VMEM((slots + 8, 256), BF16),
        pltpu.VMEM((2, 2 * HALF + 8, D), BF16),
        pltpu.VMEM((2 * HALF, H), BF16), pltpu.VMEM((2 * HALF, H), BF16), pltpu.VMEM((2 * HALF, H), BF16),
        pltpu.VMEM((GROUPS, 4, GROW, Q), BF16), pltpu.VMEM((GROUPS, 4, GROW, Q), BF16),
        pltpu.VMEM((GROUPS, 4, GROW, Q), F32),
        pltpu.VMEM((GROUPS, GROW, 256), BF16), pltpu.VMEM((GROUPS, GROW, 256), BF16),
        pltpu.VMEM((GROUPS, GROW, Q), BF16), pltpu.VMEM((GROUPS, GROW, Q), BF16),
        pltpu.VMEM((GROUPS, 4, GROW, Q), BF16),
        pltpu.VMEM((slots + 8, 128), BF16), pltpu.VMEM((slots + 8, 128), BF16),
        pltpu.VMEM((TOK, D), BF16),
        pltpu.VMEM((2, 1024, C), F32), pltpu.VMEM((1024, C), BF16), pltpu.VMEM((1024, C), BF16),
        pltpu.VMEM((1024, C), BF16), pltpu.VMEM((768, C), BF16), pltpu.VMEM((256, C), BF16), pltpu.VMEM((256, C), BF16),
        pltpu.VMEM((TOK, C), F32), pltpu.VMEM((16, C), F32), pltpu.VMEM((NX, 8, TOK), F32),
        dma((15,)), dma((2,)), dma((11,)), dma((8,)), dma((4, 4)), dma((4,)), dma((2, 4)), dma((5,)), dma((3,)), dma((4,)), dma((2,)),
    ]
    made = pl.pallas_call(
        kernel,
        out_shape=[pltpu.VMEM(*shape) for shape in shapes],
        in_specs=[hbm] * 15,
        out_specs=[vmem] * 7,
        scratch_shapes=scratch,
        compiler_params=pltpu.CompilerParams(
            collective_id=0, has_side_effects=True, vmem_limit_bytes=56 * 1024 * 1024
        ),
    )(*args[:2], args[2].T, args[3].T, *args[4:], perm, perm_t)
    return pl.pallas_call(
        finish,
        out_shape=[jax.ShapeDtypeStruct(*shape) for shape in shapes],
        in_specs=[vmem] * 7,
        out_specs=[hbm] * 7,
        scratch_shapes=[dma((7,))],
        compiler_params=pltpu.CompilerParams(vmem_limit_bytes=1024 * 1024),
    )(*made)


def solution(mesh):
    in_specs = (
        P("sp", None), P("sp", None), P("sp", None), P("sp", None),
        P("sp", None, "tp"), P("sp", None, "tp"), P("sp", "tp", None),
        P("sp", "tp"), P("sp", "tp"), P("sp", "tp"), P("sp", "tp"),
        P(None, "tp"), P("tp", None),
    )
    out_specs = (
        P("sp", None), P("sp", None, "tp"), P("sp", "tp", None),
        P("sp", "tp"), P("sp", "tp"), P("sp", "tp"), P("sp", "tp"),
    )
    return jax.shard_map(
        per_device, mesh=mesh, in_specs=in_specs, out_specs=out_specs, check_vma=False
    )
```

```python
import jax
import jax.numpy as jnp
import numpy as np
from jax import lax
from jax.experimental import pallas as pl
from jax.experimental.pallas import tpu as pltpu
from jax.sharding import PartitionSpec as P

MESH = pl.DeviceIdType.MESH
EPS = 1e-06
F32 = jnp.float32
BF16 = jnp.bfloat16

D = 2048
H = 512
Q = 512
TOK = 128
CAP = 10
NZ, NY, NX = 8, 4, 4
CHIPS = NZ * NY
MSG = 4 * CAP
GROUPS = 4
GROW = 8 * CAP
HALF = GROUPS * GROW
C = 256
Z_ORDER = (0, 1, 6, 3, 5, 4, 7, 2)
O_OFF = (2, 1, 3, 0)


def permutation(sources):
    place = np.zeros((sources * MSG, sources * MSG), np.float32)
    for part in range(4):
        for source in range(sources):
            for slot in range(CAP):
                place[(part * sources + source) * CAP + slot, source * MSG + part * CAP + slot] = 1
    return place


def nt(a, b):
    return lax.dot_general(a, b, (((1,), (1,)), ((), ())), preferred_element_type=F32)


def tn(a, b):
    return lax.dot_general(a, b, (((0,), (0,)), ((), ())), preferred_element_type=F32)


def nn(a, b):
    return jnp.dot(a, b, preferred_element_type=F32)


def m8(value, by=8):
    return pl.multiple_of(value, by)


def kernel(
    og_h, resid_h, routes_h, rw_h, wg_h, wu_h, wd_h, ogate_h, igate_h, cin_h, cout_h, taps_h, wout_h,
    perm_h, perm_t_h,
    gr_o, gup_o, gdn_o, gog_o, gig_o, gci_o, gwo_o,
    og, resid, routes, rw, ogate, igate, cin, cout, taps, wout, perm, perm_t,
    wg, wu, wd, s_buf, r_buf, xa, hid, dga, dup, ps, pr, po, ra, rb, rc, rd, cs, rt, bk, dn,
    gacc, gb, gp, gs, gy_in, gz_out, gz_in, dcv, halo, dots,
    w_sem, loc_sem, send_sem, pl_r, xr, q_r, e_r, dn_r, g_r, one_r, gm_r,
):
    s = lax.axis_index("sp")
    x = lax.axis_index("tp")
    c = s // 2
    k = s % 2
    z = c // NY
    y = c % NY
    right = (s, (x + 1) % NX)
    left = (s, (x + 3) % NX)
    far = (s, (x + 2) % NX)
    mate = (2 * c + 1 - k, x)
    before = ((s + 63) % 64, x)
    after = ((s + 1) % 64, x)
    across = ((s + 63 + 2 * k) % 64, x)

    def expert_of(i, dy):
        return ((z + NZ - Z_ORDER[i]) % NZ) * NY + (y + dy) % NY

    def place_of(i, dy):
        return i * NY + (NY - dy) % NY

    def rcopy(src, dst, ss, rs, dev):
        return pltpu.make_async_remote_copy(
            src_ref=src, dst_ref=dst, send_sem=ss, recv_sem=rs, device_id=dev, device_id_type=MESH
        )

    barrier = pltpu.get_barrier_semaphore()
    for i in range(NZ):
        for dy in range(NY):
            if i or dy:
                pl.semaphore_signal(
                    barrier, inc=1, device_id=(2 * expert_of(i, dy) + k, x), device_id_type=MESH
                )
    for dev in (right, left, far, mate, across):
        pl.semaphore_signal(barrier, inc=1, device_id=dev, device_id_type=MESH)

    loads = [
        pltpu.make_async_copy(src, dst, w_sem.at[n])
        for n, (src, dst) in enumerate(
            (
                (routes_h, routes), (rw_h, rw), (resid_h, resid), (og_h, og), (perm_h, perm),
                (wg_h.at[0], wg), (wu_h.at[0], wu), (wd_h.at[0], wd),
                (perm_t_h, perm_t), (ogate_h, ogate), (cout_h, cout), (wout_h, wout),
                (cin_h, cin), (igate_h, igate), (taps_h, taps),
            )
        )
    ]
    for copy in loads[:5]:
        copy.start()

    loads[0].wait()
    loads[1].wait()
    lanes = lax.broadcasted_iota(jnp.int32, (TOK, TOK), 1)
    subs = lax.broadcasted_iota(jnp.int32, (TOK, TOK), 0)
    eye = lanes == subs

    def column(row):
        return jnp.sum(jnp.where(eye, row.astype(F32), 0.0), axis=1, keepdims=True)

    r0 = column(routes[0:1, :])
    r1 = column(routes[1:2, :])
    w0 = column(rw[0:1, :])
    w1 = column(rw[1:2, :])
    a0 = (lanes.astype(F32) == r0).astype(F32)
    a1 = (lanes.astype(F32) == r1).astype(F32)
    earlier = (lanes < subs).astype(F32).astype(BF16)
    counts = nn(earlier, (a0 + a1).astype(BF16))
    s0 = r0 * MSG + jnp.sum(a0 * counts, axis=1, keepdims=True)
    s1 = r1 * MSG + jnp.sum(a1 * counts, axis=1, keepdims=True)
    s0_row = jnp.sum(jnp.where(eye, s0, 0.0), axis=0, keepdims=True)
    s1_row = jnp.sum(jnp.where(eye, s1, 0.0), axis=0, keepdims=True)

    loads[2].wait()
    loads[3].wait()
    rf = resid[...].astype(F32)
    inv = lax.rsqrt(jnp.mean(rf * rf, axis=-1, keepdims=True) + EPS)
    qcol = m8(x * Q, Q)
    norm_q = (resid[:, pl.ds(qcol, Q)].astype(F32) * inv).astype(BF16)
    og_q = og[:, pl.ds(qcol, Q)].astype(F32)
    w0_q = (w0 * og_q).astype(BF16)
    w1_q = (w1 * og_q).astype(BF16)
    data = jnp.concatenate(
        [
            norm_q[:, :256], norm_q[:, 256:],
            w0_q[:, :256], w1_q[:, :256], w0_q[:, 256:], w1_q[:, 256:],
        ],
        axis=0,
    )

    def build(b, carry):
        rows = (lax.broadcasted_iota(jnp.int32, (8 * MSG, TOK), 0) + b * (8 * MSG)).astype(F32)

        def hot(base):
            return (rows == base).astype(F32)

        picks = jnp.concatenate(
            [
                hot(s0_row) + hot(s1_row),
                hot(s0_row + CAP) + hot(s1_row + CAP),
                hot(s0_row + 2 * CAP), hot(s1_row + 2 * CAP),
                hot(s0_row + 3 * CAP), hot(s1_row + 3 * CAP),
            ],
            axis=1,
        ).astype(BF16)
        s_buf[pl.ds(m8(b * 8 * MSG, 8 * MSG), 8 * MSG), :] = nn(picks, data).astype(BF16)
        return carry

    for copy in loads[5:]:
        copy.start()
    lax.fori_loop(0, GROUPS, build, 0)
    loads[4].wait()

    pl.semaphore_wait(barrier, 36)

    def send_rows(i, dy):
        e = expert_of(i, dy)
        p = place_of(i, dy)
        return rcopy(
            s_buf.at[pl.ds(m8(e * MSG), MSG), :],
            r_buf.at[pl.ds(p * MSG, MSG), :],
            send_sem.at[0], pl_r.at[i], (2 * e + k, x),
        )

    own_rows = pltpu.make_async_copy(
        s_buf.at[pl.ds(m8(c * MSG), MSG), :], r_buf.at[pl.ds(0, MSG), :], loc_sem.at[0]
    )
    own_rows.start()
    for i in range(NZ):
        for dy in range(NY):
            if i or dy:
                send_rows(i, dy).start()
    own_rows.wait()

    def col(off):
        return m8(((x + off) % NX) * Q, Q)

    def xa_at(core, g, off, kind=None):
        rows = pl.ds(m8(core * HALF + g * GROW, 16), GROW)
        if kind is None:
            return xa.at[:, rows, pl.ds(col(off), Q)]
        return xa.at[kind, rows, pl.ds(col(off), Q)]

    def own_copy(n, g, half):
        block = xa.at[
            :, pl.ds(m8(k * HALF + g * GROW + half * (GROW // 2)), GROW // 2), pl.ds(qcol, Q)
        ]
        return rcopy(block, block, send_sem.at[1], xr.at[(0, 1, 3)[n], g], (right, left, mate)[n])

    def x_copy(n, g):
        block, dev = {
            3: lambda: (xa_at(k, g, 3, 0), right),
            4: lambda: (xa_at(k, g, 1, 1), left),
            5: lambda: (xa_at(k, g, 3), mate),
            6: lambda: (xa_at(k, g, 1), mate),
            7: lambda: (xa_at(k, g, 2), mate),
        }[n]()
        return rcopy(block, block, send_sem.at[1], xr.at[2 if n < 5 else 3, g], dev)

    def x_wait(n, g):
        block = (
            lambda: xa_at(k, g, 3),
            lambda: xa_at(k, g, 1),
            lambda: xa_at(k, g, 2),
            lambda: xa.at[:, pl.ds(m8((1 - k) * HALF + g * GROW, 16), GROW), :],
        )[n]()
        rcopy(block, block, send_sem.at[1], xr.at[n, g], mate).wait_recv()

    def take(block, sem):
        rcopy(block, block, sem, sem, mate).wait_recv()

    def sent(block, sem):
        rcopy(block, block, sem, sem, mate).wait_send()

    def stage_in(g):
        for half in range(2):
            base = (2 * g + half) * NY * MSG
            if half:
                take(r_buf.at[pl.ds(m8(base, NY * MSG), NY * MSG), :], pl_r.at[2 * g + 1])
            else:

                @pl.when(g == 0)
                def _():
                    take(r_buf.at[pl.ds(MSG, 3 * MSG), :], pl_r.at[0])

                @pl.when(g > 0)
                def _():
                    take(r_buf.at[pl.ds(m8(base, NY * MSG), NY * MSG), :], pl_r.at[2 * g])

            got = nn(perm[...], r_buf[pl.ds(m8(base, NY * MSG), NY * MSG), :]).astype(BF16)
            rows = pl.ds(m8(k * HALF + g * GROW + half * (GROW // 2)), GROW // 2)
            for kind in range(2):
                for part in range(2):
                    n = 2 * kind + part
                    xa[kind, rows, pl.ds(m8(qcol + part * 256, 256), 256)] = got[n * MSG : (n + 1) * MSG]
            for n in range(3):
                own_copy(n, g, half).start()

    def stage_relay(g):
        x_wait(0, g)
        x_copy(3, g).start()
        x_copy(5, g).start()
        x_wait(1, g)
        x_copy(4, g).start()
        x_copy(6, g).start()

    def stage_far(g):
        x_wait(2, g)
        x_copy(7, g).start()

    def both(buf, kind, g):
        return jnp.concatenate(
            [buf[kind, pl.ds(m8(core * HALF + g * GROW, 16), GROW), :] for core in range(2)], axis=0
        )

    def stage_compute(g):
        x_wait(3, g)
        rows_n = both(xa, 0, g)
        pre_gate = nn(rows_n, wg[...])
        pre_up = nn(rows_n, wu[...])
        d_hidden = nt(both(xa, 1, g), wd[...])
        sig = jax.nn.sigmoid(pre_gate)
        act = pre_gate * sig
        hid_v = (act * pre_up).astype(BF16)
        dg_v = (d_hidden * pre_up * sig * (1.0 + pre_gate * (1.0 - sig))).astype(BF16)
        du_v = (d_hidden * act).astype(BF16)
        for core in range(2):
            rows = pl.ds(m8(core * HALF + g * GROW, 16), GROW)
            part = slice(core * GROW, (core + 1) * GROW)
            hid[rows, :] = hid_v[part]
            dga[rows, :] = dg_v[part]
            dup[rows, :] = du_v[part]

    def mate_copy(g):
        return rcopy(ps.at[g], pr.at[g], send_sem.at[2], q_r.at[g], mate)

    def e_copy(n, g):
        src, dst, dev = (
            (cs.at[g, 0, :, pl.ds(0, 256)], ra.at[g], right),
            (cs.at[g, 0, :, pl.ds(256, 256)], rb.at[g], left),
            (cs.at[g, 1], rc.at[g], right),
            (cs.at[g, 2], rd.at[g], left),
        )[n]
        return rcopy(src, dst, send_sem.at[3], e_r.at[n // 2, g], dev)

    def back_copy(p, source):
        return rcopy(
            rt.at[pl.ds(m8(p * MSG), MSG), :],
            bk.at[pl.ds(m8(c * MSG), MSG), :],
            send_sem.at[4], one_r.at[0], (2 * source + k, x),
        )

    def source_in(g, j):
        away = 0
        for n in range(1 if j < NY else 0, GROUPS):
            away = away + Z_ORDER[2 * n + j // NY] * (1 - ((g - n) * (g - n) + 8) // 9)
        return ((z + away) % NZ) * NY + (y + j % NY) % NY

    def stage_make(g):
        d_gate = jnp.concatenate(
            [dga[pl.ds(m8(core * HALF + g * GROW, 16), GROW), :] for core in (1 - k, k)], axis=0
        )
        d_up = jnp.concatenate(
            [dup[pl.ds(m8(core * HALF + g * GROW, 16), GROW), :] for core in (1 - k, k)], axis=0
        )
        for o in range(4):
            feats = pl.ds(col(O_OFF[o]), Q)
            part = nt(d_gate, wg[feats, :]) + nt(d_up, wu[feats, :])
            ps[g, o] = part[:GROW].astype(BF16)
            po[g, o] = part[GROW:]
        mate_copy(g).start()

    def stage_first(g):
        mate_copy(g).wait_recv()
        cs[g, 0] = (po[g, 0] + pr[g, 0].astype(F32)).astype(BF16)
        e_copy(0, g).start()
        e_copy(1, g).start()

    def stage_second(g):
        take(cs.at[g, 0], e_r.at[0, g])
        total = po[g, 1] + pr[g, 1].astype(F32)
        cs[g, 1, :, 0:256] = (total[:, :256] + ra[g].astype(F32)).astype(BF16)
        cs[g, 1, :, 256:512] = total[:, 256:].astype(BF16)
        e_copy(2, g).start()
        total = po[g, 2] + pr[g, 2].astype(F32)
        cs[g, 2, :, 0:256] = total[:, :256].astype(BF16)
        cs[g, 2, :, 256:512] = (total[:, 256:] + rb[g].astype(F32)).astype(BF16)
        e_copy(3, g).start()

    def stage_back(g):
        take(cs.at[g, pl.ds(0, 2)], e_r.at[1, g])
        mine = (po[g, 3] + pr[g, 3].astype(F32) + rc[g].astype(F32) + rd[g].astype(F32)).astype(BF16)
        stacked = jnp.concatenate([mine[:, j * 128 : (j + 1) * 128] for j in range(4)], axis=0)
        rt[pl.ds(m8(g * 8 * MSG, 8 * MSG), 8 * MSG), :] = nn(perm_t[...], stacked).astype(BF16)
        for j in range(8):
            copy = back_copy(g * 8 + j, source_in(g, j))
            if j:
                copy.start()
            else:
                pl.when(g > 0)(copy.start)

    def down_step(b, carry):
        cols = pl.ds(m8(b * 512, 512), 512)
        gdn_o[0, :, cols] = tn(hid[...], xa[1, 0 : 2 * HALF, cols]).astype(BF16)
        return carry

    def up_step(b, carry):
        cols = pl.ds(m8(b * 512, 512), 512)
        gup_o[0, cols, :] = tn(xa[0, 0 : 2 * HALF, cols], dup[...]).astype(BF16)
        return carry

    def step(t, carry):
        def at(cond, stage, *g):
            pl.when(cond)(lambda: stage(*g))

        def loaded():
            for copy in loads[5:]:
                copy.wait()

        at(t < 4, stage_in, t)
        at((t >= 1) & (t < 5), stage_relay, t - 1)
        at(t == 3, loaded)
        at(t == 4, stage_first, 0)
        at((t == 2) | (t == 4) | (t == 5), stage_far, t - 2)
        at(t == 5, stage_second, 0)
        at((t >= 3) & (t < 7), stage_compute, t - 3)
        at((t == 5) | (t == 6), stage_first, t - 4)
        at(t == 6, stage_second, 1)
        at((t >= 3) & (t < 7), stage_make, t - 3)
        at(t == 3, stage_far, 1)
        at(t == 7, stage_back, 0)
        at(t == 7, stage_first, 3)
        at((t == 7) | (t == 8), stage_second, t - 5)
        at(t >= 7, stage_back, t - 6)
        return carry

    lax.fori_loop(0, GROUPS + 6, step, 0)

    own_back = pltpu.make_async_copy(
        rt.at[pl.ds(0, MSG), :], bk.at[pl.ds(m8(c * MSG), MSG), :], loc_sem.at[1]
    )
    own_back.start()
    lax.fori_loop(0, 4, up_step, 0)
    lax.fori_loop(0, 4, down_step, 0)
    own_back.wait()

    take(bk.at[pl.ds(0, (CHIPS - 1) * MSG), :], one_r.at[0])
    cols = lax.broadcasted_iota(jnp.int32, (TOK, CHIPS * MSG), 1).astype(F32)
    back = bk[pl.ds(0, CHIPS * MSG), :]

    def dn_at(off, h, rows=None):
        return dn.at[
            pl.ds(0, TOK) if rows is None else pl.ds(rows, TOK // 2),
            pl.ds(m8(((x + off) % NX) * Q + h * 256, 256), 256),
        ]

    def dn_copy(n, h):
        block, dev = (
            lambda: (dn_at(0, h), right),
            lambda: (dn_at(0, h), left),
            lambda: (dn_at(3, h, 0), right),
            lambda: (dn_at(1, h, TOK // 2), left),
        )[n]()
        return rcopy(block, block, send_sem.at[5], dn_r.at[(0, 2, 4, 4)[n] + (h if n < 2 else 0)], dev)

    for j in range(4):
        hot = ((cols == s0 + j * CAP) | (cols == s1 + j * CAP)).astype(F32).astype(BF16)
        dn[:, pl.ds(m8(qcol + j * 128, 128), 128)] = nn(hot, back).astype(BF16)

    def unit_of(feats):
        return resid[:, feats].astype(F32) * inv

    own_feats = pl.ds(qcol, Q)
    part = jnp.sum(unit_of(own_feats) * dn[:, own_feats].astype(F32), axis=1, keepdims=True)
    part = jnp.sum(jnp.where(eye, part, 0.0), axis=0, keepdims=True)
    dots[x] = jnp.broadcast_to(part, (8, TOK))
    for dev in (right, left, far):
        rcopy(dots.at[x], dots.at[x], send_sem.at[10], one_r.at[3], dev).start()
    for h in range(2):
        dn_copy(0, h).start()
        dn_copy(1, h).start()
    mixed = (ogate[...].astype(F32) * cout[...].astype(F32)).astype(BF16)
    take(dots.at[pl.ds(0, 3)], one_r.at[3])
    means = (dots[0, 0:1, :] + dots[1, 0:1, :] + dots[2, 0:1, :] + dots[3, 0:1, :]) * (1.0 / D)
    row_mean = jnp.sum(jnp.where(eye, means, 0.0), axis=1, keepdims=True)

    def quarter_rows(off):
        return pl.ds(m8(((x + off) % NX) * 256, 256), 256)

    def quarter(off, chunk):
        feats = pl.ds(col(off), Q)
        rows = quarter_rows(off)
        gr = (
            og[:, feats].astype(F32)
            + inv * (dn[:, feats].astype(F32) - unit_of(feats) * row_mean)
        ).astype(BF16)
        gr_o[:, feats] = gr
        grad_w = tn(gr, mixed).reshape(8, 2, 32, C)
        gacc[0, rows, :] = grad_w[:, 0].reshape(256, C)
        gacc[1, rows, :] = grad_w[:, 1].reshape(256, C)
        gb[rows, :] = gacc[1 - k, rows, :].astype(BF16)
        rcopy(gb.at[rows, :], gp.at[rows, :], send_sem.at[6], gm_r.at[chunk], mate).start()

    def along_y(offs, first, chunk):
        for n, off in enumerate(offs):
            rows = quarter_rows(off)
            gs[rows, :] = (gacc[k, rows, :] + gp[rows, :].astype(F32)).astype(BF16)
            for zz in range(2):
                for dy in range(1, NY):
                    there = (y + dy) % NY
                    block = ((2 * ((x + off) % NX) + zz) * NY + there) * 32
                    rcopy(
                        gs.at[pl.ds(m8(block, 32), 32), :],
                        gy_in.at[pl.ds(((dy - 1) * NZ + first + 2 * n + zz) * 32, 32), :],
                        send_sem.at[8], g_r.at[chunk], (2 * (z * NY + there) + k, x),
                    ).start()

    def along_z(offs, first):
        for n, off in enumerate(offs):
            for zz in range(2):
                there = 2 * ((x + off) % NX) + zz
                slot = (first + 2 * n + zz) * 32
                total = gs[pl.ds(m8((there * NY + y) * 32, 32), 32), :].astype(F32)
                for d in range(NY - 1):
                    total = total + gy_in[d * 256 + slot : d * 256 + slot + 32, :].astype(F32)
                gz_out[slot : slot + 32, :] = total.astype(BF16)

                @pl.when(there == z)
                def _():
                    gz_in[pl.ds(m8(z * 32, 32), 32), :] = gz_out[slot : slot + 32, :]

                @pl.when(there != z)
                def _():
                    rcopy(
                        gz_out.at[pl.ds(slot, 32), :], gz_in.at[pl.ds(m8(z * 32, 32), 32), :],
                        send_sem.at[9], g_r.at[2], (2 * (there * NY + y) + k, x),
                    ).start()

    near = (0, 3, 1)
    quarter(0, 0)
    for h in range(2):
        take(dn_at(3, h), dn_r.at[h])
        dn_copy(2, h).start()
        take(dn_at(1, h), dn_r.at[2 + h])
        dn_copy(3, h).start()
    quarter(3, 0)
    quarter(1, 0)
    take(gp.at[pl.ds(0, 768), :], gm_r.at[0])
    along_y(near, 0, 0)
    take(dn.at[:, pl.ds(col(2), Q)], dn_r.at[4])
    quarter(2, 1)

    d_mix = nt(gr_o[...], wout[...])
    d_conv = d_mix * ogate[...].astype(F32)
    dcv[...] = d_conv
    to_after = rcopy(
        dcv.at[pl.ds(TOK - 8, 8), :], halo.at[pl.ds(0, 8), :], send_sem.at[7], one_r.at[2], after
    )
    to_before = rcopy(
        dcv.at[pl.ds(0, 8), :], halo.at[pl.ds(8, 8), :], send_sem.at[7], one_r.at[2], before
    )
    to_after.start()
    to_before.start()
    gog_o[...] = (d_mix * cout[...].astype(F32)).astype(BF16)

    take(gp.at[pl.ds(0, 256), :], gm_r.at[1])
    along_y((2,), 6, 1)
    take(gy_in.at[pl.ds(0, 576), :], g_r.at[0])
    along_z(near, 0)
    take(gy_in.at[pl.ds(0, 192), :], g_r.at[1])
    along_z((2,), 6)

    take(halo, one_r.at[2])
    row = lax.broadcasted_iota(jnp.int32, (TOK, C), 0)
    next_row = jnp.where(s == 63, 0.0, halo[8:9, :])
    prev_row = jnp.where(s == 0, 0.0, halo[7:8, :])
    nxt = jnp.where(row == TOK - 1, next_row, pltpu.roll(d_conv, TOK - 1, 0))
    prv = jnp.where(row == 0, prev_row, pltpu.roll(d_conv, 1, 0))
    d_inner = taps[0:1, :] * nxt + taps[1:2, :] * d_conv + taps[2:3, :] * prv
    gig_o[...] = (d_inner * cin[...].astype(F32)).astype(BF16)
    gci_o[...] = (d_inner * igate[...].astype(F32)).astype(BF16)

    take(gz_in.at[pl.ds(0, 224), :], g_r.at[2])
    gwo_o[...] = jnp.sum(gz_in[...].reshape(NZ, 32, C).astype(F32), axis=0)

    sent(s_buf.at[pl.ds(0, (CHIPS - 1) * MSG), :], send_sem.at[0])
    sent(xa.at[:, pl.ds(0, 2 * HALF), pl.ds(0, 1792)], send_sem.at[1])
    sent(ps, send_sem.at[2])
    sent(cs.at[:, pl.ds(0, 3)], send_sem.at[3])
    sent(rt.at[pl.ds(0, (CHIPS - 1) * MSG), :], send_sem.at[4])
    sent(dn.at[:, pl.ds(0, 1536)], send_sem.at[5])
    sent(gb, send_sem.at[6])
    sent(halo, send_sem.at[7])
    sent(gy_in, send_sem.at[8])
    sent(gz_in.at[pl.ds(0, 224), :], send_sem.at[9])
    sent(dots.at[pl.ds(0, 3)], send_sem.at[10])


def finish(*refs):
    ins, outs, sems = refs[:7], refs[7:14], refs[14]
    copies = [pltpu.make_async_copy(a, b, sems.at[n]) for n, (a, b) in enumerate(zip(ins, outs))]
    for copy in copies:
        copy.start()
    for copy in copies:
        copy.wait()


def per_device(*args):
    perm = jnp.asarray(permutation(NY), BF16)
    perm_t = jnp.asarray(permutation(8).T, BF16)
    vmem = pl.BlockSpec(memory_space=pltpu.VMEM)
    hbm = pl.BlockSpec(memory_space=pl.ANY)
    dma = pltpu.SemaphoreType.DMA
    shapes = [
        ((TOK, D), BF16), ((1, D, H), BF16), ((1, H, D), BF16),
        ((TOK, C), BF16), ((TOK, C), BF16), ((TOK, C), BF16), ((32, C), F32),
    ]
    slots = CHIPS * MSG
    scratch = [
        pltpu.VMEM((TOK, D), BF16), pltpu.VMEM((TOK, D), BF16),
        pltpu.VMEM((2, TOK), jnp.int32), pltpu.VMEM((2, TOK), F32),
        pltpu.VMEM((TOK, C), BF16), pltpu.VMEM((TOK, C), BF16), pltpu.VMEM((TOK, C), BF16), pltpu.VMEM((TOK, C), BF16),
        pltpu.VMEM((3, C), F32), pltpu.VMEM((C, D), BF16),
        pltpu.VMEM((NY * MSG, NY * MSG), BF16), pltpu.VMEM((8 * MSG, 8 * MSG), BF16),
        pltpu.VMEM((D, H), BF16), pltpu.VMEM((D, H), BF16), pltpu.VMEM((H, D), BF16),
        pltpu.VMEM((slots + 8, 256), BF16), pltpu.VMEM((slots + 8, 256), BF16),
        pltpu.VMEM((2, 2 * HALF + 8, D), BF16),
        pltpu.VMEM((2 * HALF, H), BF16), pltpu.VMEM((2 * HALF, H), BF16), pltpu.VMEM((2 * HALF, H), BF16),
        pltpu.VMEM((GROUPS, 4, GROW, Q), BF16), pltpu.VMEM((GROUPS, 4, GROW, Q), BF16),
        pltpu.VMEM((GROUPS, 4, GROW, Q), F32),
        pltpu.VMEM((GROUPS, GROW, 256), BF16), pltpu.VMEM((GROUPS, GROW, 256), BF16),
        pltpu.VMEM((GROUPS, GROW, Q), BF16), pltpu.VMEM((GROUPS, GROW, Q), BF16),
        pltpu.VMEM((GROUPS, 4, GROW, Q), BF16),
        pltpu.VMEM((slots + 8, 128), BF16), pltpu.VMEM((slots + 8, 128), BF16),
        pltpu.VMEM((TOK, D), BF16),
        pltpu.VMEM((2, 1024, C), F32), pltpu.VMEM((1024, C), BF16), pltpu.VMEM((1024, C), BF16),
        pltpu.VMEM((1024, C), BF16), pltpu.VMEM((768, C), BF16), pltpu.VMEM((256, C), BF16), pltpu.VMEM((256, C), BF16),
        pltpu.VMEM((TOK, C), F32), pltpu.VMEM((16, C), F32), pltpu.VMEM((NX, 8, TOK), F32),
        dma((15,)), dma((2,)), dma((11,)), dma((8,)), dma((4, 4)), dma((4,)), dma((2, 4)), dma((5,)), dma((3,)), dma((4,)), dma((2,)),
    ]
    made = pl.pallas_call(
        kernel,
        out_shape=[pltpu.VMEM(*shape) for shape in shapes],
        in_specs=[hbm] * 15,
        out_specs=[vmem] * 7,
        scratch_shapes=scratch,
        compiler_params=pltpu.CompilerParams(
            collective_id=0, has_side_effects=True, vmem_limit_bytes=56 * 1024 * 1024
        ),
    )(*args[:2], args[2].T, args[3].T, *args[4:], perm, perm_t)
    return pl.pallas_call(
        finish,
        out_shape=[jax.ShapeDtypeStruct(*shape) for shape in shapes],
        in_specs=[vmem] * 7,
        out_specs=[hbm] * 7,
        scratch_shapes=[dma((7,))],
        compiler_params=pltpu.CompilerParams(vmem_limit_bytes=1024 * 1024),
    )(*made)


def solution(mesh):
    in_specs = (
        P("sp", None), P("sp", None), P("sp", None), P("sp", None),
        P("sp", None, "tp"), P("sp", None, "tp"), P("sp", "tp", None),
        P("sp", "tp"), P("sp", "tp"), P("sp", "tp"), P("sp", "tp"),
        P(None, "tp"), P("tp", None),
    )
    out_specs = (
        P("sp", None), P("sp", None, "tp"), P("sp", "tp", None),
        P("sp", "tp"), P("sp", "tp"), P("sp", "tp"), P("sp", "tp"),
    )
    return jax.shard_map(
        per_device, mesh=mesh, in_specs=in_specs, out_specs=out_specs, check_vma=False
    )
```

```python
import jax
import jax.numpy as jnp
import numpy as np
from jax import lax
from jax.experimental import pallas as pl
from jax.experimental.pallas import tpu as pltpu
from jax.sharding import PartitionSpec as P

MESH = pl.DeviceIdType.MESH
EPS = 1e-06
F32 = jnp.float32
BF16 = jnp.bfloat16

D = 2048
H = 512
Q = 512
TOK = 128
CAP = 10
NZ, NY, NX = 8, 4, 4
CHIPS = NZ * NY
MSG = 4 * CAP
GROUPS = 4
GROW = 8 * CAP
HALF = GROUPS * GROW
C = 256
Z_ORDER = (0, 1, 6, 3, 5, 4, 7, 2)
O_OFF = (2, 1, 3, 0)


def permutation(sources):
    place = np.zeros((sources * MSG, sources * MSG), np.float32)
    for part in range(4):
        for source in range(sources):
            for slot in range(CAP):
                place[(part * sources + source) * CAP + slot, source * MSG + part * CAP + slot] = 1
    return place


def nt(a, b):
    return lax.dot_general(a, b, (((1,), (1,)), ((), ())), preferred_element_type=F32)


def tn(a, b):
    return lax.dot_general(a, b, (((0,), (0,)), ((), ())), preferred_element_type=F32)


def nn(a, b):
    return jnp.dot(a, b, preferred_element_type=F32)


def m8(value, by=8):
    return pl.multiple_of(value, by)


def kernel(
    og_h, resid_h, routes_h, rw_h, wg_h, wu_h, wd_h, ogate_h, igate_h, cin_h, cout_h, taps_h, wout_h,
    perm_h, perm_t_h,
    gr_o, gup_o, gdn_o, gog_o, gig_o, gci_o, gwo_o,
    og, resid, routes, rw, ogate, igate, cin, cout, taps, wout, perm, perm_t,
    wg, wu, wd, s_buf, r_buf, xa, hid, dga, dup, ps, pr, po, ra, rb, rc, rd, cs, rt, bk, dn,
    gacc, gb, gp, gs, gy_in, gz_out, gz_in, dcv, halo, dots,
    w_sem, loc_sem, send_sem, pl_r, xr, q_r, e_r, dn_r, g_r, one_r, gm_r,
):
    s = lax.axis_index("sp")
    x = lax.axis_index("tp")
    c = s // 2
    k = s % 2
    z = c // NY
    y = c % NY
    right = (s, (x + 1) % NX)
    left = (s, (x + 3) % NX)
    far = (s, (x + 2) % NX)
    mate = (2 * c + 1 - k, x)
    before = ((s + 63) % 64, x)
    after = ((s + 1) % 64, x)
    across = ((s + 63 + 2 * k) % 64, x)

    def expert_of(i, dy):
        return ((z + NZ - Z_ORDER[i]) % NZ) * NY + (y + dy) % NY

    def place_of(i, dy):
        return i * NY + (NY - dy) % NY

    def rcopy(src, dst, ss, rs, dev):
        return pltpu.make_async_remote_copy(
            src_ref=src, dst_ref=dst, send_sem=ss, recv_sem=rs, device_id=dev, device_id_type=MESH
        )

    barrier = pltpu.get_barrier_semaphore()
    for i in range(NZ):
        for dy in range(NY):
            if i or dy:
                pl.semaphore_signal(
                    barrier, inc=1, device_id=(2 * expert_of(i, dy) + k, x), device_id_type=MESH
                )
    for dev in (right, left, far, mate, across):
        pl.semaphore_signal(barrier, inc=1, device_id=dev, device_id_type=MESH)

    loads = [
        pltpu.make_async_copy(src, dst, w_sem.at[n])
        for n, (src, dst) in enumerate(
            (
                (routes_h, routes), (rw_h, rw), (resid_h, resid), (og_h, og), (perm_h, perm),
                (wg_h.at[0], wg), (wu_h.at[0], wu), (wd_h.at[0], wd),
                (perm_t_h, perm_t), (ogate_h, ogate), (cout_h, cout), (wout_h, wout),
                (cin_h, cin), (igate_h, igate), (taps_h, taps),
            )
        )
    ]
    for copy in loads[:5]:
        copy.start()

    loads[0].wait()
    loads[1].wait()
    lanes = lax.broadcasted_iota(jnp.int32, (TOK, TOK), 1)
    subs = lax.broadcasted_iota(jnp.int32, (TOK, TOK), 0)
    eye = lanes == subs

    def column(row):
        return jnp.sum(jnp.where(eye, row.astype(F32), 0.0), axis=1, keepdims=True)

    r0 = column(routes[0:1, :])
    r1 = column(routes[1:2, :])
    w0 = column(rw[0:1, :])
    w1 = column(rw[1:2, :])
    a0 = (lanes.astype(F32) == r0).astype(F32)
    a1 = (lanes.astype(F32) == r1).astype(F32)
    earlier = (lanes < subs).astype(F32).astype(BF16)
    counts = nn(earlier, (a0 + a1).astype(BF16))
    s0 = r0 * MSG + jnp.sum(a0 * counts, axis=1, keepdims=True)
    s1 = r1 * MSG + jnp.sum(a1 * counts, axis=1, keepdims=True)
    s0_row = jnp.sum(jnp.where(eye, s0, 0.0), axis=0, keepdims=True)
    s1_row = jnp.sum(jnp.where(eye, s1, 0.0), axis=0, keepdims=True)

    loads[2].wait()
    loads[3].wait()
    rf = resid[...].astype(F32)
    inv = lax.rsqrt(jnp.mean(rf * rf, axis=-1, keepdims=True) + EPS)
    qcol = m8(x * Q, Q)
    norm_q = (resid[:, pl.ds(qcol, Q)].astype(F32) * inv).astype(BF16)
    og_q = og[:, pl.ds(qcol, Q)].astype(F32)
    w0_q = (w0 * og_q).astype(BF16)
    w1_q = (w1 * og_q).astype(BF16)
    data = jnp.concatenate(
        [
            norm_q[:, :256], norm_q[:, 256:],
            w0_q[:, :256], w1_q[:, :256], w0_q[:, 256:], w1_q[:, 256:],
        ],
        axis=0,
    )

    def build(b, carry):
        rows = (lax.broadcasted_iota(jnp.int32, (8 * MSG, TOK), 0) + b * (8 * MSG)).astype(F32)

        def hot(base):
            return (rows == base).astype(F32)

        picks = jnp.concatenate(
            [
                hot(s0_row) + hot(s1_row),
                hot(s0_row + CAP) + hot(s1_row + CAP),
                hot(s0_row + 2 * CAP), hot(s1_row + 2 * CAP),
                hot(s0_row + 3 * CAP), hot(s1_row + 3 * CAP),
            ],
            axis=1,
        ).astype(BF16)
        s_buf[pl.ds(m8(b * 8 * MSG, 8 * MSG), 8 * MSG), :] = nn(picks, data).astype(BF16)
        return carry

    for copy in loads[5:]:
        copy.start()
    lax.fori_loop(0, GROUPS, build, 0)
    loads[4].wait()

    pl.semaphore_wait(barrier, 36)

    def send_rows(i, dy):
        e = expert_of(i, dy)
        p = place_of(i, dy)
        return rcopy(
            s_buf.at[pl.ds(m8(e * MSG), MSG), :],
            r_buf.at[pl.ds(p * MSG, MSG), :],
            send_sem.at[0], pl_r.at[i], (2 * e + k, x),
        )

    own_rows = pltpu.make_async_copy(
        s_buf.at[pl.ds(m8(c * MSG), MSG), :], r_buf.at[pl.ds(0, MSG), :], loc_sem.at[0]
    )
    own_rows.start()
    for i in range(NZ):
        for dy in (2, 1, 3, 0):
            if i or dy:
                send_rows(i, dy).start()
    own_rows.wait()

    def col(off):
        return m8(((x + off) % NX) * Q, Q)

    def xa_at(core, g, off, kind=None):
        rows = pl.ds(m8(core * HALF + g * GROW, 16), GROW)
        if kind is None:
            return xa.at[:, rows, pl.ds(col(off), Q)]
        return xa.at[kind, rows, pl.ds(col(off), Q)]

    def own_copy(n, g, half):
        block = xa.at[
            :, pl.ds(m8(k * HALF + g * GROW + half * (GROW // 2)), GROW // 2), pl.ds(qcol, Q)
        ]
        return rcopy(block, block, send_sem.at[1], xr.at[(0, 1, 3)[n], g], (right, left, mate)[n])

    def x_copy(n, g):
        block, dev = {
            3: lambda: (xa_at(k, g, 3, 0), right),
            4: lambda: (xa_at(k, g, 1, 1), left),
            5: lambda: (xa_at(k, g, 3), mate),
            6: lambda: (xa_at(k, g, 1), mate),
            7: lambda: (xa_at(k, g, 2), mate),
        }[n]()
        return rcopy(block, block, send_sem.at[1], xr.at[2 if n < 5 else 3, g], dev)

    def x_wait(n, g):
        block = (
            lambda: xa_at(k, g, 3),
            lambda: xa_at(k, g, 1),
            lambda: xa_at(k, g, 2),
            lambda: xa.at[:, pl.ds(m8((1 - k) * HALF + g * GROW, 16), GROW), :],
        )[n]()
        rcopy(block, block, send_sem.at[1], xr.at[n, g], mate).wait_recv()

    def take(block, sem):
        rcopy(block, block, sem, sem, mate).wait_recv()

    def sent(block, sem):
        rcopy(block, block, sem, sem, mate).wait_send()

    def stage_in(g):
        for half in range(2):
            base = (2 * g + half) * NY * MSG
            if half:
                take(r_buf.at[pl.ds(m8(base, NY * MSG), NY * MSG), :], pl_r.at[2 * g + 1])
            else:

                @pl.when(g == 0)
                def _():
                    take(r_buf.at[pl.ds(MSG, 3 * MSG), :], pl_r.at[0])

                @pl.when(g > 0)
                def _():
                    take(r_buf.at[pl.ds(m8(base, NY * MSG), NY * MSG), :], pl_r.at[2 * g])

            got = nn(perm[...], r_buf[pl.ds(m8(base, NY * MSG), NY * MSG), :]).astype(BF16)
            rows = pl.ds(m8(k * HALF + g * GROW + half * (GROW // 2)), GROW // 2)
            for kind in range(2):
                for part in range(2):
                    n = 2 * kind + part
                    xa[kind, rows, pl.ds(m8(qcol + part * 256, 256), 256)] = got[n * MSG : (n + 1) * MSG]
            for n in range(3):
                own_copy(n, g, half).start()

    def stage_relay(g):
        x_wait(0, g)
        x_copy(3, g).start()
        x_copy(5, g).start()
        x_wait(1, g)
        x_copy(4, g).start()
        x_copy(6, g).start()

    def stage_far(g):
        x_wait(2, g)
        x_copy(7, g).start()

    def both(buf, kind, g):
        return jnp.concatenate(
            [buf[kind, pl.ds(m8(core * HALF + g * GROW, 16), GROW), :] for core in range(2)], axis=0
        )

    def stage_compute(g):
        x_wait(3, g)
        rows_n = both(xa, 0, g)
        pre_gate = nn(rows_n, wg[...])
        pre_up = nn(rows_n, wu[...])
        d_hidden = nt(both(xa, 1, g), wd[...])
        sig = jax.nn.sigmoid(pre_gate)
        act = pre_gate * sig
        hid_v = (act * pre_up).astype(BF16)
        dg_v = (d_hidden * pre_up * sig * (1.0 + pre_gate * (1.0 - sig))).astype(BF16)
        du_v = (d_hidden * act).astype(BF16)
        for core in range(2):
            rows = pl.ds(m8(core * HALF + g * GROW, 16), GROW)
            part = slice(core * GROW, (core + 1) * GROW)
            hid[rows, :] = hid_v[part]
            dga[rows, :] = dg_v[part]
            dup[rows, :] = du_v[part]

    def mate_copy(g):
        return rcopy(ps.at[g], pr.at[g], send_sem.at[2], q_r.at[g], mate)

    def e_copy(n, g):
        src, dst, dev = (
            (cs.at[g, 0, :, pl.ds(0, 256)], ra.at[g], right),
            (cs.at[g, 0, :, pl.ds(256, 256)], rb.at[g], left),
            (cs.at[g, 1], rc.at[g], right),
            (cs.at[g, 2], rd.at[g], left),
        )[n]
        return rcopy(src, dst, send_sem.at[3], e_r.at[n // 2, g], dev)

    def back_copy(p, source):
        return rcopy(
            rt.at[pl.ds(m8(p * MSG), MSG), :],
            bk.at[pl.ds(m8(c * MSG), MSG), :],
            send_sem.at[4], one_r.at[0], (2 * source + k, x),
        )

    def source_in(g, j):
        away = 0
        for n in range(1 if j < NY else 0, GROUPS):
            away = away + Z_ORDER[2 * n + j // NY] * (1 - ((g - n) * (g - n) + 8) // 9)
        return ((z + away) % NZ) * NY + (y + j % NY) % NY

    def stage_make(g):
        d_gate = jnp.concatenate(
            [dga[pl.ds(m8(core * HALF + g * GROW, 16), GROW), :] for core in (1 - k, k)], axis=0
        )
        d_up = jnp.concatenate(
            [dup[pl.ds(m8(core * HALF + g * GROW, 16), GROW), :] for core in (1 - k, k)], axis=0
        )
        for o in range(4):
            feats = pl.ds(col(O_OFF[o]), Q)
            part = nt(d_gate, wg[feats, :]) + nt(d_up, wu[feats, :])
            ps[g, o] = part[:GROW].astype(BF16)
            po[g, o] = part[GROW:]
        mate_copy(g).start()

    def stage_first(g):
        mate_copy(g).wait_recv()
        cs[g, 0] = (po[g, 0] + pr[g, 0].astype(F32)).astype(BF16)
        e_copy(0, g).start()
        e_copy(1, g).start()

    def stage_second(g):
        take(cs.at[g, 0], e_r.at[0, g])
        total = po[g, 1] + pr[g, 1].astype(F32)
        cs[g, 1, :, 0:256] = (total[:, :256] + ra[g].astype(F32)).astype(BF16)
        cs[g, 1, :, 256:512] = total[:, 256:].astype(BF16)
        e_copy(2, g).start()
        total = po[g, 2] + pr[g, 2].astype(F32)
        cs[g, 2, :, 0:256] = total[:, :256].astype(BF16)
        cs[g, 2, :, 256:512] = (total[:, 256:] + rb[g].astype(F32)).astype(BF16)
        e_copy(3, g).start()

    def stage_back(g):
        take(cs.at[g, pl.ds(0, 2)], e_r.at[1, g])
        mine = (po[g, 3] + pr[g, 3].astype(F32) + rc[g].astype(F32) + rd[g].astype(F32)).astype(BF16)
        stacked = jnp.concatenate([mine[:, j * 128 : (j + 1) * 128] for j in range(4)], axis=0)
        rt[pl.ds(m8(g * 8 * MSG, 8 * MSG), 8 * MSG), :] = nn(perm_t[...], stacked).astype(BF16)
        for j in range(8):
            copy = back_copy(g * 8 + j, source_in(g, j))
            if j:
                copy.start()
            else:
                pl.when(g > 0)(copy.start)

    def down_step(b, carry):
        cols = pl.ds(m8(b * 512, 512), 512)
        gdn_o[0, :, cols] = tn(hid[...], xa[1, 0 : 2 * HALF, cols]).astype(BF16)
        return carry

    def up_step(b, carry):
        cols = pl.ds(m8(b * 512, 512), 512)
        gup_o[0, cols, :] = tn(xa[0, 0 : 2 * HALF, cols], dup[...]).astype(BF16)
        return carry

    def step(t, carry):
        def at(cond, stage, *g):
            pl.when(cond)(lambda: stage(*g))

        def loaded():
            for copy in loads[5:]:
                copy.wait()

        at(t < 4, stage_in, t)
        at((t >= 1) & (t < 5), stage_relay, t - 1)
        at(t == 3, loaded)
        at(t == 4, stage_first, 0)
        at((t == 2) | (t == 4) | (t == 5), stage_far, t - 2)
        at(t == 5, stage_second, 0)
        at((t >= 3) & (t < 7), stage_compute, t - 3)
        at((t == 5) | (t == 6), stage_first, t - 4)
        at(t == 6, stage_second, 1)
        at((t >= 3) & (t < 7), stage_make, t - 3)
        at(t == 3, stage_far, 1)
        at(t == 7, stage_back, 0)
        at(t == 7, stage_first, 3)
        at((t == 7) | (t == 8), stage_second, t - 5)
        at(t >= 7, stage_back, t - 6)
        return carry

    lax.fori_loop(0, GROUPS + 6, step, 0)

    own_back = pltpu.make_async_copy(
        rt.at[pl.ds(0, MSG), :], bk.at[pl.ds(m8(c * MSG), MSG), :], loc_sem.at[1]
    )
    own_back.start()
    lax.fori_loop(0, 4, up_step, 0)
    lax.fori_loop(0, 4, down_step, 0)
    own_back.wait()

    take(bk.at[pl.ds(0, (CHIPS - 1) * MSG), :], one_r.at[0])
    cols = lax.broadcasted_iota(jnp.int32, (TOK, CHIPS * MSG), 1).astype(F32)
    back = bk[pl.ds(0, CHIPS * MSG), :]

    def dn_at(off, h, rows=None):
        return dn.at[
            pl.ds(0, TOK) if rows is None else pl.ds(rows, TOK // 2),
            pl.ds(m8(((x + off) % NX) * Q + h * 256, 256), 256),
        ]

    def dn_copy(n, h):
        block, dev = (
            lambda: (dn_at(0, h), right),
            lambda: (dn_at(0, h), left),
            lambda: (dn_at(3, h, 0), right),
            lambda: (dn_at(1, h, TOK // 2), left),
        )[n]()
        return rcopy(block, block, send_sem.at[5], dn_r.at[(0, 2, 4, 4)[n] + (h if n < 2 else 0)], dev)

    for j in range(4):
        hot = ((cols == s0 + j * CAP) | (cols == s1 + j * CAP)).astype(F32).astype(BF16)
        dn[:, pl.ds(m8(qcol + j * 128, 128), 128)] = nn(hot, back).astype(BF16)

    def unit_of(feats):
        return resid[:, feats].astype(F32) * inv

    own_feats = pl.ds(qcol, Q)
    part = jnp.sum(unit_of(own_feats) * dn[:, own_feats].astype(F32), axis=1, keepdims=True)
    part = jnp.sum(jnp.where(eye, part, 0.0), axis=0, keepdims=True)
    dots[x] = jnp.broadcast_to(part, (8, TOK))
    for dev in (right, left, far):
        rcopy(dots.at[x], dots.at[x], send_sem.at[10], one_r.at[3], dev).start()
    for h in range(2):
        dn_copy(0, h).start()
        dn_copy(1, h).start()
    mixed = (ogate[...].astype(F32) * cout[...].astype(F32)).astype(BF16)
    take(dots.at[pl.ds(0, 3)], one_r.at[3])
    means = (dots[0, 0:1, :] + dots[1, 0:1, :] + dots[2, 0:1, :] + dots[3, 0:1, :]) * (1.0 / D)
    row_mean = jnp.sum(jnp.where(eye, means, 0.0), axis=1, keepdims=True)

    def quarter_rows(off):
        return pl.ds(m8(((x + off) % NX) * 256, 256), 256)

    def quarter(off, chunk):
        feats = pl.ds(col(off), Q)
        rows = quarter_rows(off)
        gr = (
            og[:, feats].astype(F32)
            + inv * (dn[:, feats].astype(F32) - unit_of(feats) * row_mean)
        ).astype(BF16)
        gr_o[:, feats] = gr
        grad_w = tn(gr, mixed).reshape(8, 2, 32, C)
        gacc[0, rows, :] = grad_w[:, 0].reshape(256, C)
        gacc[1, rows, :] = grad_w[:, 1].reshape(256, C)
        gb[rows, :] = gacc[1 - k, rows, :].astype(BF16)
        rcopy(gb.at[rows, :], gp.at[rows, :], send_sem.at[6], gm_r.at[chunk], mate).start()

    def along_y(offs, first, chunk):
        for n, off in enumerate(offs):
            rows = quarter_rows(off)
            gs[rows, :] = (gacc[k, rows, :] + gp[rows, :].astype(F32)).astype(BF16)
            for zz in range(2):
                for dy in (2, 1, 3):
                    there = (y + dy) % NY
                    block = ((2 * ((x + off) % NX) + zz) * NY + there) * 32
                    rcopy(
                        gs.at[pl.ds(m8(block, 32), 32), :],
                        gy_in.at[pl.ds(((dy - 1) * NZ + first + 2 * n + zz) * 32, 32), :],
                        send_sem.at[8], g_r.at[chunk], (2 * (z * NY + there) + k, x),
                    ).start()

    def along_z(offs, first):
        for n, off in enumerate(offs):
            for zz in range(2):
                there = 2 * ((x + off) % NX) + zz
                slot = (first + 2 * n + zz) * 32
                total = gs[pl.ds(m8((there * NY + y) * 32, 32), 32), :].astype(F32)
                for d in range(NY - 1):
                    total = total + gy_in[d * 256 + slot : d * 256 + slot + 32, :].astype(F32)
                gz_out[slot : slot + 32, :] = total.astype(BF16)

                @pl.when(there == z)
                def _():
                    gz_in[pl.ds(m8(z * 32, 32), 32), :] = gz_out[slot : slot + 32, :]

                @pl.when(there != z)
                def _():
                    rcopy(
                        gz_out.at[pl.ds(slot, 32), :], gz_in.at[pl.ds(m8(z * 32, 32), 32), :],
                        send_sem.at[9], g_r.at[2], (2 * (there * NY + y) + k, x),
                    ).start()

    near = (0, 3, 1)
    quarter(0, 0)
    for h in range(2):
        take(dn_at(3, h), dn_r.at[h])
        dn_copy(2, h).start()
        take(dn_at(1, h), dn_r.at[2 + h])
        dn_copy(3, h).start()
    quarter(3, 0)
    quarter(1, 0)
    take(gp.at[pl.ds(0, 768), :], gm_r.at[0])
    along_y(near, 0, 0)
    take(dn.at[:, pl.ds(col(2), Q)], dn_r.at[4])
    quarter(2, 1)

    d_mix = nt(gr_o[...], wout[...])
    d_conv = d_mix * ogate[...].astype(F32)
    dcv[...] = d_conv
    to_after = rcopy(
        dcv.at[pl.ds(TOK - 8, 8), :], halo.at[pl.ds(0, 8), :], send_sem.at[7], one_r.at[2], after
    )
    to_before = rcopy(
        dcv.at[pl.ds(0, 8), :], halo.at[pl.ds(8, 8), :], send_sem.at[7], one_r.at[2], before
    )
    to_after.start()
    to_before.start()
    gog_o[...] = (d_mix * cout[...].astype(F32)).astype(BF16)

    take(gp.at[pl.ds(0, 256), :], gm_r.at[1])
    along_y((2,), 6, 1)
    take(gy_in.at[pl.ds(0, 576), :], g_r.at[0])
    along_z(near, 0)
    take(gy_in.at[pl.ds(0, 192), :], g_r.at[1])
    along_z((2,), 6)

    take(halo, one_r.at[2])
    row = lax.broadcasted_iota(jnp.int32, (TOK, C), 0)
    next_row = jnp.where(s == 63, 0.0, halo[8:9, :])
    prev_row = jnp.where(s == 0, 0.0, halo[7:8, :])
    nxt = jnp.where(row == TOK - 1, next_row, pltpu.roll(d_conv, TOK - 1, 0))
    prv = jnp.where(row == 0, prev_row, pltpu.roll(d_conv, 1, 0))
    d_inner = taps[0:1, :] * nxt + taps[1:2, :] * d_conv + taps[2:3, :] * prv
    gig_o[...] = (d_inner * cin[...].astype(F32)).astype(BF16)
    gci_o[...] = (d_inner * igate[...].astype(F32)).astype(BF16)

    take(gz_in.at[pl.ds(0, 224), :], g_r.at[2])
    gwo_o[...] = jnp.sum(gz_in[...].reshape(NZ, 32, C).astype(F32), axis=0)

    sent(s_buf.at[pl.ds(0, (CHIPS - 1) * MSG), :], send_sem.at[0])
    sent(xa.at[:, pl.ds(0, 2 * HALF), pl.ds(0, 1792)], send_sem.at[1])
    sent(ps, send_sem.at[2])
    sent(cs.at[:, pl.ds(0, 3)], send_sem.at[3])
    sent(rt.at[pl.ds(0, (CHIPS - 1) * MSG), :], send_sem.at[4])
    sent(dn.at[:, pl.ds(0, 1536)], send_sem.at[5])
    sent(gb, send_sem.at[6])
    sent(halo, send_sem.at[7])
    sent(gy_in, send_sem.at[8])
    sent(gz_in.at[pl.ds(0, 224), :], send_sem.at[9])
    sent(dots.at[pl.ds(0, 3)], send_sem.at[10])


def finish(*refs):
    ins, outs, sems = refs[:7], refs[7:14], refs[14]
    copies = [pltpu.make_async_copy(a, b, sems.at[n]) for n, (a, b) in enumerate(zip(ins, outs))]
    for copy in copies:
        copy.start()
    for copy in copies:
        copy.wait()


def per_device(*args):
    perm = jnp.asarray(permutation(NY), BF16)
    perm_t = jnp.asarray(permutation(8).T, BF16)
    vmem = pl.BlockSpec(memory_space=pltpu.VMEM)
    hbm = pl.BlockSpec(memory_space=pl.ANY)
    dma = pltpu.SemaphoreType.DMA
    shapes = [
        ((TOK, D), BF16), ((1, D, H), BF16), ((1, H, D), BF16),
        ((TOK, C), BF16), ((TOK, C), BF16), ((TOK, C), BF16), ((32, C), F32),
    ]
    slots = CHIPS * MSG
    scratch = [
        pltpu.VMEM((TOK, D), BF16), pltpu.VMEM((TOK, D), BF16),
        pltpu.VMEM((2, TOK), jnp.int32), pltpu.VMEM((2, TOK), F32),
        pltpu.VMEM((TOK, C), BF16), pltpu.VMEM((TOK, C), BF16), pltpu.VMEM((TOK, C), BF16), pltpu.VMEM((TOK, C), BF16),
        pltpu.VMEM((3, C), F32), pltpu.VMEM((C, D), BF16),
        pltpu.VMEM((NY * MSG, NY * MSG), BF16), pltpu.VMEM((8 * MSG, 8 * MSG), BF16),
        pltpu.VMEM((D, H), BF16), pltpu.VMEM((D, H), BF16), pltpu.VMEM((H, D), BF16),
        pltpu.VMEM((slots + 8, 256), BF16), pltpu.VMEM((slots + 8, 256), BF16),
        pltpu.VMEM((2, 2 * HALF + 8, D), BF16),
        pltpu.VMEM((2 * HALF, H), BF16), pltpu.VMEM((2 * HALF, H), BF16), pltpu.VMEM((2 * HALF, H), BF16),
        pltpu.VMEM((GROUPS, 4, GROW, Q), BF16), pltpu.VMEM((GROUPS, 4, GROW, Q), BF16),
        pltpu.VMEM((GROUPS, 4, GROW, Q), F32),
        pltpu.VMEM((GROUPS, GROW, 256), BF16), pltpu.VMEM((GROUPS, GROW, 256), BF16),
        pltpu.VMEM((GROUPS, GROW, Q), BF16), pltpu.VMEM((GROUPS, GROW, Q), BF16),
        pltpu.VMEM((GROUPS, 4, GROW, Q), BF16),
        pltpu.VMEM((slots + 8, 128), BF16), pltpu.VMEM((slots + 8, 128), BF16),
        pltpu.VMEM((TOK, D), BF16),
        pltpu.VMEM((2, 1024, C), F32), pltpu.VMEM((1024, C), BF16), pltpu.VMEM((1024, C), BF16),
        pltpu.VMEM((1024, C), BF16), pltpu.VMEM((768, C), BF16), pltpu.VMEM((256, C), BF16), pltpu.VMEM((256, C), BF16),
        pltpu.VMEM((TOK, C), F32), pltpu.VMEM((16, C), F32), pltpu.VMEM((NX, 8, TOK), F32),
        dma((15,)), dma((2,)), dma((11,)), dma((8,)), dma((4, 4)), dma((4,)), dma((2, 4)), dma((5,)), dma((3,)), dma((4,)), dma((2,)),
    ]
    made = pl.pallas_call(
        kernel,
        out_shape=[pltpu.VMEM(*shape) for shape in shapes],
        in_specs=[hbm] * 15,
        out_specs=[vmem] * 7,
        scratch_shapes=scratch,
        compiler_params=pltpu.CompilerParams(
            collective_id=0, has_side_effects=True, vmem_limit_bytes=56 * 1024 * 1024
        ),
    )(*args[:2], args[2].T, args[3].T, *args[4:], perm, perm_t)
    return pl.pallas_call(
        finish,
        out_shape=[jax.ShapeDtypeStruct(*shape) for shape in shapes],
        in_specs=[vmem] * 7,
        out_specs=[hbm] * 7,
        scratch_shapes=[dma((7,))],
        compiler_params=pltpu.CompilerParams(vmem_limit_bytes=1024 * 1024),
    )(*made)


def solution(mesh):
    in_specs = (
        P("sp", None), P("sp", None), P("sp", None), P("sp", None),
        P("sp", None, "tp"), P("sp", None, "tp"), P("sp", "tp", None),
        P("sp", "tp"), P("sp", "tp"), P("sp", "tp"), P("sp", "tp"),
        P(None, "tp"), P("tp", None),
    )
    out_specs = (
        P("sp", None), P("sp", None, "tp"), P("sp", "tp", None),
        P("sp", "tp"), P("sp", "tp"), P("sp", "tp"), P("sp", "tp"),
    )
    return jax.shard_map(
        per_device, mesh=mesh, in_specs=in_specs, out_specs=out_specs, check_vma=False
    )
```
